32 devices in a mesh: fs: 8 (over z, y), tp: 4 (over x, core).
Axes of the slice: x: 2, y: 2, z: 4, core: 2. Of those that a mesh axis runs over, the one named last changes fastest.
Arguments:
- tokens: bfloat16 [8192, 2048], P('fs'), may hold values from -6 to 6
- norm_gain: float32 [2048], replicated, may hold values from 0.1 to 1.9
- gate_weight: bfloat16 [2048, 4096], P('fs', 'tp'), may hold values from -0.125 to 0.125
- up_weight: bfloat16 [2048, 4096], P('fs', 'tp'), may hold values from -0.125 to 0.125
- down_weight: bfloat16 [4096, 2048], P('tp', 'fs'), may hold values from -2 to 2
- out_gain: float32 [2048], P('tp'), may hold values from 0.1 to 1.9
Outputs:
- result: bfloat16 [8192, 2048], P('fs', 'tp')
The draws below stay inside these ranges and needn't reach their ends.
All inputs are finite; a program needn't handle non-finite values.
Results may differ from the reference program's by a relative error of at most 0.014.
Values may be sent and summed in bfloat16 or wider, within the bound.
A program may use at most 64 MiB of HBM per device.

```python
import jax
import jax.numpy as jnp
from jax import lax

D = 2048
FF = 4096
TOK_DEV = 1024
TOKENS = 8192
N_FS = 8
N_TP = 4


def draw_down_weight(key, part):
    first_key, second_key = jax.random.split(jax.random.fold_in(key, 17))
    group_scales = jnp.exp(jax.random.uniform(second_key, (16,), jnp.float32, -0.9, 0.9))
    column_scale = jnp.repeat(group_scales, D // 16)
    base = jnp.clip(jax.random.normal(first_key, (FF, D), jnp.float32), -4.0, 4.0)
    values = jnp.clip(base * FF ** (-0.5) * column_scale[None, :], -2.0, 2.0)
    return values.astype(jnp.bfloat16)


def shard_levels(key, shape, cuts, low, largest):
    def one(position, parts):
        steps = jax.random.uniform(jax.random.fold_in(jax.random.fold_in(key, 6), position), (parts,), jnp.float32, low / len(cuts), largest / len(cuts))
        return jnp.repeat(jnp.exp(steps), shape[position] // parts).reshape((-1,) + (1,) * (len(shape) - position - 1))

    gain = one(*cuts[0])
    for cut in cuts[1:]:
        gain = gain * one(*cut)
    return gain


def normal_values(own_key, shape, spread, reach, cuts=(), dtype=jnp.bfloat16):
    drawn = spread * jax.random.normal(own_key, shape, jnp.float32)
    if cuts:
        drawn = drawn * shard_levels(own_key, shape, cuts, -0.22, 0.18)
    return jnp.clip(drawn, -reach, reach).astype(dtype)


def setup_inputs(seed: int = 0) -> dict:
    key_list = jax.random.split(jax.random.key(seed), 7)
    return {
        "tokens": normal_values(key_list[0], (TOKENS, D), 1.0, 6.0, ((0, 8),)),
        "norm_gain": jnp.clip(1.0 + 0.18 * jax.random.normal(key_list[1], (D,), jnp.float32), 0.1, 1.9),
        "gate_weight": normal_values(key_list[2], (D, FF), D ** -0.5, 0.125, ((0, 8), (1, 4))),
        "up_weight": normal_values(key_list[3], (D, FF), D ** -0.5, 0.125, ((0, 8), (1, 4))),
        "down_weight": draw_down_weight(jax.random.fold_in(key_list[6], 71), 0),
        "out_gain": jnp.clip(1.0 + 0.18 * jax.random.normal(key_list[5], (D,), jnp.float32), 0.1, 1.9),
    }


EPSILON = 1e-06

def reference(tokens, norm_gain, gate_weight, up_weight, down_weight, out_gain):
    width = FF // N_TP
    down_blocks = down_weight.reshape(N_TP, width, D)

    def one_block(rows):
        values = rows.astype(jnp.float32)
        normed = (values * lax.rsqrt(lax.optimization_barrier(jnp.mean(values * values, axis=1, keepdims=True)) + EPSILON) * norm_gain.astype(jnp.float32)).astype(jnp.bfloat16)
        gate_proj = jnp.dot(normed, gate_weight, preferred_element_type=jnp.float32)
        up_proj = jnp.dot(normed, up_weight, preferred_element_type=jnp.float32)
        hidden = (jax.nn.silu(gate_proj) * up_proj).astype(jnp.bfloat16)
        branch = jnp.zeros((rows.shape[0], D), jnp.float32)
        for index in range(N_TP):
            piece = jnp.dot(hidden[:, index * width:(index + 1) * width], down_blocks[index], preferred_element_type=jnp.float32).astype(jnp.bfloat16)
            branch = branch + lax.optimization_barrier(piece).astype(jnp.float32)
        mean_square = lax.optimization_barrier(jnp.mean(branch * branch, axis=1, keepdims=True))
        return (branch * lax.rsqrt(mean_square + EPSILON) * out_gain.astype(jnp.float32)).astype(jnp.bfloat16)
    blocks = tokens.reshape(N_FS, TOK_DEV, D)
    return lax.map(one_block, blocks).reshape(TOKENS, D)
```

```python
import functools

import jax
import jax.numpy as jnp
from jax import lax
from jax.experimental import pallas as pl
from jax.experimental.pallas import tpu as pltpu
from jax.sharding import PartitionSpec as P

EPSILON = 1e-06
MESH = pl.DeviceIdType.MESH
PIECES = 2
COLUMN_TILE = 256
TOKEN_PIECES = 4
LAG = 6


def ring_layout(n, n_tp):
    ny = max(n_tp // 2, 1)
    if n % ny or (n // ny) % 2:
        ny = 1
    nz, rest = n // ny, max(ny - 1, 1)

    def position(fs):
        z, y = fs // ny, fs % ny
        k = nz - 1 - z
        odd = k % 2
        back = nz + k * rest + (1 - odd) * (y - 1) + odd * (ny - 1 - y)
        return jnp.where(y == 0, z, back)

    def index(pos):
        q = jnp.maximum(pos - nz, 0)
        k, r = q // rest, q % rest
        odd = k % 2
        back = (nz - 1 - k) * ny + (1 - odd) * (1 + r) + odd * (ny - 1 - r)
        return jnp.where(pos < nz, pos * ny, back)

    return position, index


def kernel(
    n, n_tp, tokens_hbm, norm_gain, gate_hbm, up_hbm, down_hbm, out_gain, out_ref,
    tok, normed, gate, up, down, gate_acc, up_acc, hidden, parts, sib, far, own, sq, sq_all,
    local_sem, ring_send, ring_recv, sib_send, sib_recv, far_send, far_recv, sq_send, sq_recv,
):
    half = n // 2
    nx, cuts = n_tp // 2, down.shape[0] // n
    nb = n * cuts // n_tp
    n_tok, d_model = tok.shape
    rows_in = gate.shape[1]
    n_hid, width = down.shape[1], down.shape[2]
    piece = n_tok // PIECES
    position, index = ring_layout(n, n_tp)
    fs, tp = lax.axis_index("fs"), lax.axis_index("tp")
    x, core = tp // 2, tp % 2
    me = position(fs)
    block_of = {}
    for h in range(half + 1):
        block_of[0, h] = index((me + n - h) % n)
        block_of[1, h] = index((me + h) % n)
    target = (block_of[1, 1], block_of[0, 1])
    sibling = x * 2 + 1 - core

    barrier = pltpu.get_barrier_semaphore()
    for fs_id in target:
        pl.semaphore_signal(barrier, inc=1, device_id={"fs": fs_id}, device_id_type=MESH)
    for d in range(1, n_tp):
        pl.semaphore_signal(
            barrier, inc=1, device_id={"tp": (tp + d) % n_tp}, device_id_type=MESH
        )
    loads = [
        pltpu.make_async_copy(tokens_hbm, tok, local_sem.at[0]),
        pltpu.make_async_copy(gate_hbm, gate.at[fs], local_sem.at[1]),
        pltpu.make_async_copy(up_hbm, up.at[fs], local_sem.at[2]),
    ]
    for j in range(cuts):
        cols = pl.ds(j * width, width)
        loads.append(
            pltpu.make_async_copy(
                down_hbm.at[:, cols], down.at[fs * cuts + j], local_sem.at[3 + j]
            )
        )
    for load in loads:
        load.start()
    pl.semaphore_wait(barrier, 2 + n_tp - 1)

    def view(c, b, h, way):
        if c < 2:
            ref = (gate, up)[c]
            if h == half:
                return ref.at[b, pl.ds(way * (rows_in // 2), rows_in // 2)]
            return ref.at[b]
        if h == half:
            return down.at[b * cuts + c - 2, pl.ds(way * (n_hid // 2), n_hid // 2)]
        return down.at[b * cuts + c - 2]

    def ring_copy(c, way, h, b, first=False):
        dst = view(c, b, h, way)
        src = (gate_hbm, up_hbm)[c] if first and c < 2 else dst
        return pltpu.make_async_remote_copy(
            src_ref=src,
            dst_ref=dst,
            send_sem=ring_send.at[way, h - 1, c],
            recv_sem=ring_recv.at[way, h - 1, c],
            device_id={"fs": target[way]},
            device_id_type=MESH,
        )

    sends = []

    def send(c, way, h):
        copy = ring_copy(c, way, h, block_of[way, h - 1], h == 1)
        copy.start()
        sends.append(copy)

    def arrive(c, way, h):
        ring_copy(c, way, h, block_of[way, h]).wait_recv()

    for c in (0, 1):
        for way in (0, 1):
            send(c, way, 1)

    loads[0].wait()
    tile = min(128, n_tok)

    @pl.loop(0, n_tok // tile)
    def _(i):
        rows = pl.ds(pl.multiple_of(i * tile, tile), tile)
        v = tok[rows, :].astype(jnp.float32)
        r = lax.rsqrt(jnp.mean(v * v, axis=1, keepdims=True) + EPSILON)
        out = (v * r * norm_gain[...]).astype(jnp.bfloat16)
        for j in range(n):
            normed[j, rows, :] = out[:, j * rows_in:(j + 1) * rows_in]

    def accumulate(b, mode):
        n_col = gate.shape[2]
        step = min(COLUMN_TILE, n_col)

        @pl.loop(0, n_col // step)
        def _(i):
            cols = pl.ds(pl.multiple_of(i * step, step), step)
            a = normed[b]
            g = jnp.dot(a, gate[b, :, cols], preferred_element_type=jnp.float32)
            u = jnp.dot(a, up[b, :, cols], preferred_element_type=jnp.float32)
            if mode != "first":
                g = g + gate_acc[:, cols]
                u = u + up_acc[:, cols]
            if mode == "last":
                hidden[:, cols] = (g * (1.0 / (1.0 + jnp.exp(-g))) * u).astype(jnp.bfloat16)
            else:
                gate_acc[:, cols] = g
                up_acc[:, cols] = u

    loads[1].wait()
    loads[2].wait()
    accumulate(fs, "first")
    for load in loads[3:]:
        load.wait()

    for h in range(1, half + 1):
        for c in (0, 1):
            for way in (0, 1):
                arrive(c, way, h)
                if h < half:
                    send(c, way, h + 1)
        if h == half - 1:
            for j in range(cuts):
                for way in (0, 1):
                    send(2 + j, way, 1)
        if h < half:
            accumulate(block_of[0, h], "mid")
            accumulate(block_of[1, h], "mid")
        else:
            accumulate(block_of[0, h], "last")

    def owner(b):
        t = b // nb
        return t // 2, t % 2, b % nb

    def piece_rows(q):
        return pl.ds(pl.multiple_of(q * piece, piece), piece)

    def sib_copy(b, slot, q):
        return pltpu.make_async_remote_copy(
            src_ref=parts.at[b, piece_rows(q)],
            dst_ref=sib.at[slot, piece_rows(q)],
            send_sem=sib_send.at[slot, q],
            recv_sem=sib_recv.at[slot, q],
            device_id={"tp": sibling},
            device_id_type=MESH,
        )

    def far_copy(b, x_to, x_from, k, q):
        return pltpu.make_async_remote_copy(
            src_ref=parts.at[b, piece_rows(q)],
            dst_ref=far.at[x_from, k, piece_rows(q)],
            send_sem=far_send.at[x_to * nb + k, q],
            recv_sem=far_recv.at[x_from, k, q],
            device_id={"tp": x_to * 2 + core},
            device_id_type=MESH,
        )

    def multiply(b):
        x_to, core_to, k = owner(b)

        @pl.loop(0, PIECES)
        def _(q):
            rows = piece_rows(q)
            parts[b, rows, :] = jnp.dot(
                hidden[rows, :], down[b], preferred_element_type=jnp.float32
            ).astype(jnp.bfloat16)

            @pl.when(core_to != core)
            def _():
                sib_copy(b, x_to * nb + k, q).start()

    def reduce(b):
        x_to, core_to, k = owner(b)

        @pl.when((core_to == core) & (x_to != x))
        def _():
            @pl.loop(0, PIECES)
            def _(q):
                rows = piece_rows(q)
                slot = x_to * nb + k
                sib_copy(b, slot, q).wait_recv()
                parts[b, rows, :] = (
                    parts[b, rows, :].astype(jnp.float32) + sib[slot, rows, :].astype(jnp.float32)
                ).astype(jnp.bfloat16)
                far_copy(b, x_to, x, k, q).start()

    ready = [fs * cuts + j for j in range(cuts)]
    for h in range(1, half + 1):
        for j in range(cuts):
            for way in (0, 1):
                arrive(2 + j, way, h)
                if h < half:
                    send(2 + j, way, h + 1)
            for way in (0, 1) if h < half else (0,):
                ready.append(block_of[way, h] * cuts + j)
            for b in ready:
                multiply(b)
            for b in ready:
                reduce(b)
            ready = []

    @pl.loop(0, PIECES)
    def _(q):
        rows = piece_rows(q)
        squares = jnp.zeros((piece, 1), jnp.float32)
        for k in range(nb):
            b, slot = tp * nb + k, x * nb + k
            v = parts[b, rows, :].astype(jnp.float32)
            sib_copy(b, slot, q).wait_recv()
            v = v + sib[slot, rows, :].astype(jnp.float32)
            for d in range(1, nx):
                x_from = (x + d) % nx
                far_copy(b, x, x_from, k, q).wait_recv()
                v = v + far[x_from, k, rows, :].astype(jnp.float32)
            own[k, rows, :] = v
            squares = squares + jnp.sum(v * v, axis=1, keepdims=True)
        sq[q] = jnp.transpose(jnp.broadcast_to(squares, (piece, 128)))[0:8, :]

    def sq_copy(to, slot):
        return pltpu.make_async_remote_copy(
            src_ref=sq,
            dst_ref=sq_all.at[slot],
            send_sem=sq_send.at[to],
            recv_sem=sq_recv.at[slot],
            device_id={"tp": to},
            device_id_type=MESH,
        )

    others = [(tp + d) % n_tp for d in range(1, n_tp)]
    for t in others:
        sq_copy(t, tp).start()
    for t in others:
        sq_copy(t, t).wait_recv()

    @pl.loop(0, PIECES)
    def _(q):
        rows = piece_rows(q)
        total = sq[q]
        for t in others:
            total = total + sq_all[t, q]
        r = lax.rsqrt(total / d_model + EPSILON)
        r = jnp.transpose(jnp.broadcast_to(r[0:1, :], (128, piece)))[:, 0:1]
        for k in range(nb):
            cols = slice(k * width, (k + 1) * width)
            out_ref[rows, cols] = (own[k, rows, :] * r * out_gain[:, cols]).astype(jnp.bfloat16)

    for t in others:
        sq_copy(t, tp).wait_send()
    for copy in sends:
        copy.wait_send()

    @pl.loop(0, PIECES)
    def _(q):
        for slot in range(nx * nb):
            sib_copy(slot, slot, q).wait_send()
        for d in range(1, nx):
            for k in range(nb):
                far_copy(k, (x + d) % nx, x, k, q).wait_send()


def body(n, n_tp, tokens, norm_gain, gate_weight, up_weight, down_weight, out_gain):
    n_tok, d_model = tokens.shape
    rows_in, n_hid = gate_weight.shape
    cuts = max(down_weight.shape[1] // 128, 1)
    width = down_weight.shape[1] // cuts
    half, nx, nb = n // 2, n_tp // 2, n * cuts // n_tp
    piece = n_tok // PIECES
    bf16, f32 = jnp.bfloat16, jnp.float32
    dma = pltpu.SemaphoreType.DMA
    hbm = pl.BlockSpec(memory_space=pl.ANY)
    vmem = pl.BlockSpec(memory_space=pltpu.VMEM)
    return pl.pallas_call(
        functools.partial(kernel, n, n_tp),
        out_shape=jax.ShapeDtypeStruct((n_tok, out_gain.shape[0]), bf16),
        in_specs=[hbm, vmem, hbm, hbm, hbm, vmem],
        out_specs=vmem,
        scratch_shapes=[
            pltpu.VMEM((n_tok, d_model), bf16),
            pltpu.VMEM((n, n_tok, rows_in), bf16),
            pltpu.VMEM((n, rows_in, n_hid), bf16),
            pltpu.VMEM((n, rows_in, n_hid), bf16),
            pltpu.VMEM((n * cuts, n_hid, width), bf16),
            pltpu.VMEM((n_tok, n_hid), f32),
            pltpu.VMEM((n_tok, n_hid), f32),
            pltpu.VMEM((n_tok, n_hid), bf16),
            pltpu.VMEM((n * cuts, n_tok, width), bf16),
            pltpu.VMEM((nx * nb, n_tok, width), bf16),
            pltpu.VMEM((nx, nb, n_tok, width), bf16),
            pltpu.VMEM((nb, n_tok, width), f32),
            pltpu.VMEM((PIECES, 8, piece), f32),
            pltpu.VMEM((n_tp, PIECES, 8, piece), f32),
            dma((3 + cuts,)),
            dma((2, half, 2 + cuts)),
            dma((2, half, 2 + cuts)),
            dma((nx * nb, PIECES)),
            dma((nx * nb, PIECES)),
            dma((nx * nb, PIECES)),
            dma((nx, nb, PIECES)),
            dma((n_tp,)),
            dma((n_tp,)),
        ],
        compiler_params=pltpu.CompilerParams(
            collective_id=0, has_side_effects=True, vmem_limit_bytes=62 * 1024 * 1024
        ),
        name="ffn_ring",
    )(tokens, norm_gain[None, :], gate_weight, up_weight, down_weight, out_gain[None, :])


def line_order(k, nz):
    others = [s for s in range(nz) if s != k]
    return sorted(others, key=lambda s: (abs(s - k), abs(2 * s - nz + 1)))


def inward_order(k, nz):
    out = line_order(k, nz)
    if k in (0, nz - 1):
        out[0], out[1] = out[1], out[0]
    return out


def line_kernel(
    n, n_tp, tokens_hbm, norm_gain, gate_hbm, up_hbm, down_hbm, out_gain, out_ref,
    tok, normed, gate, up, down, gate_acc, up_acc, hidden, parts, sib, near, far, own, squares, sq, sq_all,
    local_sem, y_send, y_recv, z_send, z_recv, tok_send, tok_recv,
    sib_send, sib_recv, near_send, near_recv, far_send, far_recv, sq_send, sq_recv,
):
    nz = n // 2
    cuts = down.shape[0] // n
    nb = n * cuts // n_tp
    n_own, d_model = tok.shape
    rows_in, n_hid = gate.shape[1], gate.shape[2]
    width = down.shape[2]
    quarter = n_own // n_tp
    small = quarter // TOKEN_PIECES
    half_rows = n_own // PIECES
    fs, tp = lax.axis_index("fs"), lax.axis_index("tp")
    z, y = fs // 2, fs % 2
    x, core = tp // 2, tp % 2
    fs_y = z * 2 + 1 - y
    sibling, across = x * 2 + 1 - core, (1 - x) * 2 + core
    has_next = (z < nz - 1, z > 0)
    inner = (z > 0) & (z < nz - 1)
    outer = jnp.logical_not(inner)
    inward = jnp.where(z < nz // 2, 0, 1)

    barrier = pltpu.get_barrier_semaphore()
    pl.semaphore_signal(barrier, inc=1, device_id={"fs": fs_y}, device_id_type=MESH)
    for d in range(1, n_tp):
        pl.semaphore_signal(
            barrier, inc=1, device_id={"tp": (tp + d) % n_tp}, device_id_type=MESH
        )
    for way in (0, 1):

        @pl.when(has_next[way])
        def _():
            to = {"fs": fs + 2 - 4 * way}
            pl.semaphore_signal(barrier, inc=1, device_id=to, device_id_type=MESH)

    keep = pl.ds(pl.multiple_of(y * n_hid, n_hid), n_hid)
    give = pl.ds(pl.multiple_of((1 - y) * n_hid, n_hid), n_hid)
    loads = [
        pltpu.make_async_copy(tokens_hbm, tok, local_sem.at[0]),
        pltpu.make_async_copy(gate_hbm.at[:, keep], gate.at[fs], local_sem.at[1]),
        pltpu.make_async_copy(up_hbm.at[:, keep], up.at[fs], local_sem.at[2]),
    ]
    for j in range(cuts):
        cols = pl.ds(j * width, width)
        loads.append(
            pltpu.make_async_copy(
                down_hbm.at[keep, cols], down.at[fs * cuts + j], local_sem.at[3 + j]
            )
        )
    for load in loads:
        load.start()
    pl.semaphore_wait(barrier, n_tp + (z > 0).astype(jnp.int32) + (z < nz - 1).astype(jnp.int32))

    def shard(layer, other):
        return layer * 2 + (1 - y if other else y)

    def view(p, layer):
        if p < 4:
            return (gate, up)[p % 2].at[shard(layer, p // 2)]
        j = p - 4
        return down.at[layer * 2 * cuts + j]

    def z_copy(p, way, h, layer, src=None):
        dst = view(p, layer)
        return pltpu.make_async_remote_copy(
            src_ref=dst if src is None else src,
            dst_ref=dst,
            send_sem=z_send.at[way, h - 1, p],
            recv_sem=z_recv.at[way, h - 1, p],
            device_id={"fs": fs + 2 - 4 * way},
            device_id_type=MESH,
        )

    def send_own(p, where=None):
        src = (gate_hbm, up_hbm)[p].at[:, keep] if p < 2 else None
        for way in (0, 1):

            @pl.when(has_next[way] if where is None else has_next[way] & where(way))
            def _():
                z_copy(p, way, 1, z, src).start()

    order = [line_order(k, nz) for k in range(nz)]

    def pick(values):
        out = jnp.int32(values[0])
        for k in range(1, nz):
            out = jnp.where(z == k, values[k], out)
        return out

    sources = []
    for i in range(nz - 1):
        layer = pick([order[k][i] for k in range(nz)])
        way = pick([int(order[k][i] > k) for k in range(nz)])
        h = pick([abs(order[k][i] - k) for k in range(nz)])
        onward = pick([int(0 < k < nz - 1) for k in range(nz)]) == 1
        sources.append((layer, way, h, onward))

    def receive(i, p):
        layer, way, h, onward = sources[i]
        z_copy(p, way, h, layer).wait_recv()

        @pl.when(onward)
        def _():
            z_copy(p, way, h + 1, layer).start()

    def take(j):
        for i in range(nz - 1):
            receive(i, 4 + j)
            if i == 0:
                send_own(4 + j, lambda way: inward != way)

    def y_copy(p):
        if p < 2:
            src, dst = (gate_hbm, up_hbm)[p].at[:, give], (gate, up)[p]
            src, got = src, (gate, up)[p].at[fs_y]
            dst = (gate, up)[p].at[fs]
        elif p < 2 + cuts:
            j = p - 2
            src = down_hbm.at[give, pl.ds(j * width, width)]
            dst = down.at[fs * cuts + j]
        else:
            rows = token_rows(y, tp, p - 2 - cuts)
            src = dst = normed.at[:, rows]
        return pltpu.make_async_remote_copy(
            src_ref=src,
            dst_ref=dst,
            send_sem=y_send.at[p],
            recv_sem=y_recv.at[p],
            device_id={"fs": fs_y},
            device_id_type=MESH,
        )

    def token_rows(y_of, t, p):
        start = y_of * n_own + t * quarter + p * small
        return pl.ds(pl.multiple_of(start, small), small)

    def token_copy(kind, t, p, to):
        part = normed.at[:, token_rows(1 - y, t, p)]
        return pltpu.make_async_remote_copy(
            src_ref=part,
            dst_ref=part,
            send_sem=tok_send.at[kind, p],
            recv_sem=tok_recv.at[kind, p],
            device_id={"tp": to},
            device_id_type=MESH,
        )

    for p in (0, 1):
        send_own(p)
    for p in (0, 1):
        y_copy(p).start()

    loads[0].wait()
    tile = min(128, n_own)
    tiles = n_own // tile
    own_tiles = quarter // tile

    def normalize(i):
        rows = pl.ds(pl.multiple_of(i * tile, tile), tile)
        rows_to = pl.ds(pl.multiple_of(y * n_own + i * tile, tile), tile)
        v = tok[rows, :].astype(jnp.float32)
        r = lax.rsqrt(jnp.mean(v * v, axis=1, keepdims=True) + EPSILON)
        out = (v * r * norm_gain[...]).astype(jnp.bfloat16)
        for j in range(n):
            normed[j, rows_to, :] = out[:, j * rows_in:(j + 1) * rows_in]

    @pl.loop(0, own_tiles)
    def _(i):
        normalize(tp * own_tiles + i)

    for p in range(TOKEN_PIECES):
        y_copy(2 + cuts + p).start()
    for j in range(cuts):
        y_copy(2 + j).start()

    def accumulate(c, b, y_of, mode="mid"):
        weight, acc = (gate, up)[c], (gate_acc, up_acc)[c]
        step = min(COLUMN_TILE, n_hid)
        n_col = n_hid // step

        def part(half, i):
            rows = pl.ds(pl.multiple_of(half * n_own, n_own), n_own)
            cols = pl.ds(pl.multiple_of(i * step, step), step)
            v = jnp.dot(normed[b, rows, :], weight[b, :, cols], preferred_element_type=jnp.float32)
            if mode != "first":
                v = v + acc[rows, cols]
            if mode == "last":
                g = gate_acc[rows, cols]
                hidden[rows, cols] = (g * (1.0 / (1.0 + jnp.exp(-g))) * v).astype(jnp.bfloat16)
            else:
                acc[rows, cols] = v

        @pl.loop(0, n_col if y_of is not None else 2 * n_col)
        def _(i):
            part(*((y_of, i) if y_of is not None else (i // n_col, i % n_col)))

    def tokens_in(p):
        y_copy(2 + cuts + p).wait_recv()
        token_copy(0, tp, p, across).start()
        token_copy(1, tp, p, sibling).start()

    def tokens_on(p):
        token_copy(0, across, p, across).wait_recv()
        token_copy(2, across, p, sibling).start()

    @pl.loop(own_tiles, tiles // 2)
    def _(i):
        normalize((tp * own_tiles + i) % tiles)

    y_copy(0).wait_recv()
    send_own(2)

    @pl.loop(tiles // 2, tiles)
    def _(i):
        normalize((tp * own_tiles + i) % tiles)

    for load in loads[1:]:
        load.wait()
    y_copy(1).wait_recv()
    send_own(3)
    for p in (0, 1):
        receive(0, p)
    for c in (0, 1):
        accumulate(c, fs, y, "first")
    for p in range(TOKEN_PIECES // 2):
        tokens_in(p)
    for c in (0, 1):
        accumulate(c, fs_y, y)
    for p in (2, 3):
        receive(0, p)

    @pl.when(inner)
    def _():
        for i in range(1, nz - 2):
            for p in range(4):
                receive(i, p)

    for p in range(TOKEN_PIECES // 2, TOKEN_PIECES):
        tokens_in(p)
        tokens_on(p - TOKEN_PIECES // 2)
    for p in (0, 1):
        accumulate(p, shard(sources[0][0], 0), y)
    for j in range(cuts):
        y_copy(2 + j).wait_recv()
    for j in range(2 * cuts):
        send_own(4 + j, lambda way: outer)
    for j in range(2 * cuts):
        send_own(4 + j, lambda way: inner & (inward == way))
    for p in range(TOKEN_PIECES // 2, TOKEN_PIECES):
        tokens_on(p)
    for p in (0, 1):
        accumulate(p, shard(sources[0][0], 1), y)

    @pl.when(outer)
    def _():
        for i in range(1, nz - 2):
            for p in range(4):
                receive(i, p)

    for p in range(TOKEN_PIECES):
        token_copy(1, sibling, p, sibling).wait_recv()
        token_copy(2, across + 1 - 2 * core, p, sibling).wait_recv()

    last = nz - 2

    def receive_if(where, p):
        @pl.when(where)
        def _():
            receive(last, p)

    for c in (0, 1):
        accumulate(c, fs, 1 - y, "first")
        accumulate(c, fs_y, 1 - y)
        for p in (0, 1):
            accumulate(c, shard(sources[0][0], p), 1 - y)
    receive_if(inner, 0)
    for i in range(1, nz - 2):
        for p in (0, 1):
            accumulate(p, shard(sources[i][0], 0), None)
    receive_if(inner, 1)
    for i in range(1, nz - 2):
        for p in (0, 1):
            accumulate(p, shard(sources[i][0], 1), None)
    receive_if(outer, 0)
    accumulate(0, shard(sources[last][0], 0), None)
    receive_if(inner, 2)
    receive_if(outer, 1)
    accumulate(1, shard(sources[last][0], 0), None)
    receive_if(inner, 3)
    receive_if(outer, 2)
    accumulate(0, shard(sources[last][0], 1), None)
    receive_if(outer, 3)

    @pl.when(inner)
    def _():
        take(0)

    accumulate(1, shard(sources[last][0], 1), None, "last")

    def owner(b):
        t = b // nb
        return t // 2, t % 2, b % nb

    def block_rows(q):
        return pl.ds(pl.multiple_of(q * n_own, n_own), n_own)

    def sib_copy(b, slot, q):
        return pltpu.make_async_remote_copy(
            src_ref=parts.at[b, block_rows(q)],
            dst_ref=sib.at[slot, block_rows(q)],
            send_sem=sib_send.at[slot, q],
            recv_sem=sib_recv.at[slot, q],
            device_id={"tp": sibling},
            device_id_type=MESH,
        )

    def near_copy(b, q, slot, to):
        return pltpu.make_async_remote_copy(
            src_ref=parts.at[b, block_rows(q)],
            dst_ref=near.at[slot],
            send_sem=near_send.at[slot],
            recv_sem=near_recv.at[slot],
            device_id=to,
            device_id_type=MESH,
        )

    def far_copy(b, q, k, to):
        return pltpu.make_async_remote_copy(
            src_ref=parts.at[b, block_rows(q)],
            dst_ref=far.at[k],
            send_sem=far_send.at[k],
            recv_sem=far_recv.at[k],
            device_id=to,
            device_id_type=MESH,
        )

    to_y, to_x = {"fs": fs_y}, {"tp": across}

    def multiply(b):
        x_to, core_to, k = owner(b)

        @pl.loop(0, 2)
        def _(q):
            rows = block_rows(q)
            parts[b, rows, :] = jnp.dot(
                hidden[rows, :], down[b], preferred_element_type=jnp.float32
            ).astype(jnp.bfloat16)

            @pl.when(core_to != core)
            def _():
                sib_copy(b, x_to * nb + k, q).start()

    def fold(b, slot, q, extra=None):
        rows = block_rows(q)
        sib_copy(b, slot, q).wait_recv()
        v = parts[b, rows, :].astype(jnp.float32) + sib[slot, rows, :].astype(jnp.float32)
        if extra is not None:
            v = v + near[extra].astype(jnp.float32)
        parts[b, rows, :] = v.astype(jnp.bfloat16)

    def reduce(b, y_first):
        x_to, core_to, k = owner(b)
        slot = x_to * nb + k
        if y_first:

            @pl.when(core_to == core)
            def _():
                fold(b, slot, 1 - y)
                near_copy(b, 1 - y, slot, to_y).start()

        else:

            @pl.when((core_to == core) & (x_to != x))
            def _():
                @pl.loop(0, 2)
                def _(i):
                    q = jnp.where(i == 0, 1 - y, y)
                    fold(b, slot, q)
                    near_copy(b, q, q * nb + k, to_x).start()

    def pass_on(b, y_first):
        x_to, core_to, k = owner(b)
        slot = x_to * nb + k
        if y_first:

            @pl.when((core_to == core) & (x_to != x))
            def _():
                near_copy(b, y, slot, to_y).wait_recv()
                fold(b, slot, y, slot)
                far_copy(b, y, k, to_x).start()

        else:

            @pl.when((core_to == core) & (x_to == x))
            def _():
                q = 1 - y
                near_copy(b, q, q * nb + k, to_x).wait_recv()
                fold(b, slot, q, q * nb + k)
                far_copy(b, q, k, to_y).start()

    final_order = [[k] + inward_order(k, nz) for k in range(nz)]
    steps = []

    def run(step):
        m = len(steps)
        b, kind = step
        steps.append(step)
        multiply(b)
        if m >= 1:
            reduce(*steps[m - 1])
        if m >= LAG:
            pass_on(*steps[m - LAG])

    for j in range(2 * cuts):
        if j + 1 < 2 * cuts:

            @pl.when(inner)
            def _():
                take(j + 1)

        for i in range(nz):
            layer = pick([final_order[k][i] for k in range(nz)])
            if i:
                way = pick([int(final_order[k][i] > k) for k in range(nz)])
                h = pick([abs(final_order[k][i] - k) for k in range(nz)])

                @pl.when(outer)
                def _():
                    z_copy(4 + j, way, h, layer).wait_recv()

            run((layer * 2 * cuts + j, j % 2 == 1))
    reduce(*steps[-1])
    for step in steps[-LAG:]:
        pass_on(*step)

    def piece_rows(q):
        return pl.ds(pl.multiple_of(q * half_rows, half_rows), half_rows)

    for k in range(nb):
        slot = (x if k % 2 == 1 else y) * nb + k
        sib_copy(0, x * nb + k, y).wait_recv()
        near_copy(0, 0, slot, to_x).wait_recv()
        far_copy(0, 0, k, to_x).wait_recv()

        @pl.loop(0, n_own // tile)
        def _(i):
            rows = pl.ds(pl.multiple_of(i * tile, tile), tile)
            mine = pl.ds(pl.multiple_of(y * n_own + i * tile, tile), tile)
            v = parts[tp * nb + k, mine, :].astype(jnp.float32)
            v = v + sib[x * nb + k, mine, :].astype(jnp.float32)
            v = v + near[slot, rows, :].astype(jnp.float32)
            v = v + far[k, rows, :].astype(jnp.float32)
            own[k, rows, :] = v
            squares[rows, :] = v * v if k == 0 else squares[rows, :] + v * v

    for q in range(PIECES):
        total = jnp.sum(squares[piece_rows(q), :], axis=1, keepdims=True)
        sq[q] = jnp.transpose(jnp.broadcast_to(total, (half_rows, 128)))[0:8, :]

    def sq_copy(to, slot):
        return pltpu.make_async_remote_copy(
            src_ref=sq,
            dst_ref=sq_all.at[slot],
            send_sem=sq_send.at[to],
            recv_sem=sq_recv.at[slot],
            device_id={"tp": to},
            device_id_type=MESH,
        )

    others = [(tp + d) % n_tp for d in range(1, n_tp)]
    for t in others:
        sq_copy(t, tp).start()
    for t in others:
        sq_copy(t, t).wait_recv()

    @pl.loop(0, PIECES)
    def _(q):
        rows = piece_rows(q)
        total = sq[q]
        for t in others:
            total = total + sq_all[t, q]
        r = lax.rsqrt(total / d_model + EPSILON)
        r = jnp.transpose(jnp.broadcast_to(r[0:1, :], (128, half_rows)))[:, 0:1]
        for k in range(nb):
            cols = slice(k * width, (k + 1) * width)
            out_ref[rows, cols] = (own[k, rows, :] * r * out_gain[:, cols]).astype(jnp.bfloat16)

    for t in others:
        sq_copy(t, tp).wait_send()
    for p in range(2 + cuts + TOKEN_PIECES):
        y_copy(p).wait_send()
    for p in range(TOKEN_PIECES):
        token_copy(0, tp, p, across).wait_send()
        token_copy(1, tp, p, sibling).wait_send()
        token_copy(2, across, p, sibling).wait_send()
    for p in range(4 + 2 * cuts):
        for way in (0, 1):

            @pl.when(has_next[way])
            def _():
                z_copy(p, way, 1, z).wait_send()

        for layer, way, h, onward in sources:

            @pl.when(onward)
            def _():
                z_copy(p, way, h + 1, layer).wait_send()

    @pl.loop(0, 2)
    def _(q):
        for x_to in (0, 1):
            for k in range(nb):
                sib_copy(0, x_to * nb + k, q).wait_send()

    for k in range(nb):
        far_copy(0, 0, k, to_x).wait_send()
        for q in (0, 1):
            near_copy(0, 0, q * nb + k, to_x).wait_send()


def line_body(n, n_tp, tokens, norm_gain, gate_weight, up_weight, down_weight, out_gain):
    n_own, d_model = tokens.shape
    rows_in, n_hid = gate_weight.shape[0], gate_weight.shape[1] // 2
    cuts = max(down_weight.shape[1] // 128, 1)
    width = down_weight.shape[1] // cuts
    nz, nb = n // 2, n * cuts // n_tp
    n_tok = 2 * n_own
    bf16, f32 = jnp.bfloat16, jnp.float32
    dma = pltpu.SemaphoreType.DMA
    hbm = pl.BlockSpec(memory_space=pl.ANY)
    vmem = pl.BlockSpec(memory_space=pltpu.VMEM)
    return pl.pallas_call(
        functools.partial(line_kernel, n, n_tp),
        out_shape=jax.ShapeDtypeStruct((n_own, out_gain.shape[0]), bf16),
        in_specs=[hbm, vmem, hbm, hbm, hbm, vmem],
        out_specs=vmem,
        scratch_shapes=[
            pltpu.VMEM((n_own, d_model), bf16),
            pltpu.VMEM((n, n_tok, rows_in), bf16),
            pltpu.VMEM((n, rows_in, n_hid), bf16),
            pltpu.VMEM((n, rows_in, n_hid), bf16),
            pltpu.VMEM((n * cuts, n_hid, width), bf16),
            pltpu.VMEM((n_tok, n_hid), f32),
            pltpu.VMEM((n_tok, n_hid), f32),
            pltpu.VMEM((n_tok, n_hid), bf16),
            pltpu.VMEM((n * cuts, n_tok, width), bf16),
            pltpu.VMEM((2 * nb, n_tok, width), bf16),
            pltpu.VMEM((2 * nb, n_own, width), bf16),
            pltpu.VMEM((nb, n_own, width), bf16),
            pltpu.VMEM((nb, n_own, width), f32),
            pltpu.VMEM((n_own, width), f32),
            pltpu.VMEM((PIECES, 8, n_own // PIECES), f32),
            pltpu.VMEM((n_tp, PIECES, 8, n_own // PIECES), f32),
            dma((3 + cuts,)),
            dma((2 + cuts + TOKEN_PIECES,)),
            dma((2 + cuts + TOKEN_PIECES,)),
            dma((2, nz - 1, 4 + 2 * cuts)),
            dma((2, nz - 1, 4 + 2 * cuts)),
            dma((3, TOKEN_PIECES)),
            dma((3, TOKEN_PIECES)),
            dma((2 * nb, 2)),
            dma((2 * nb, 2)),
            dma((2 * nb,)),
            dma((2 * nb,)),
            dma((nb,)),
            dma((nb,)),
            dma((n_tp,)),
            dma((n_tp,)),
        ],
        compiler_params=pltpu.CompilerParams(
            collective_id=0, has_side_effects=True, vmem_limit_bytes=62 * 1024 * 1024
        ),
        name="ffn_line",
    )(tokens, norm_gain[None, :], gate_weight, up_weight, down_weight, out_gain[None, :])


def solution(mesh):
    n, n_tp = mesh.shape["fs"], mesh.shape["tp"]
    paired = n_tp == 4 and n % 2 == 0 and n // 2 > 2
    return jax.shard_map(
        functools.partial(line_body if paired else body, n, n_tp),
        mesh=mesh,
        in_specs=(P("fs", None), P(), P("fs", "tp"), P("fs", "tp"), P("tp", "fs"), P("tp")),
        out_specs=P("fs", "tp"),
        check_vma=False,
    )
```

```python
import functools

import jax
import jax.numpy as jnp
from jax import lax
from jax.experimental import pallas as pl
from jax.experimental.pallas import tpu as pltpu
from jax.sharding import PartitionSpec as P

EPSILON = 1e-06
MESH = pl.DeviceIdType.MESH
PIECES = 2
COLUMN_TILE = 256
TOKEN_PIECES = 4
LAG = 5


def ring_layout(n, n_tp):
    ny = max(n_tp // 2, 1)
    if n % ny or (n // ny) % 2:
        ny = 1
    nz, rest = n // ny, max(ny - 1, 1)

    def position(fs):
        z, y = fs // ny, fs % ny
        k = nz - 1 - z
        odd = k % 2
        back = nz + k * rest + (1 - odd) * (y - 1) + odd * (ny - 1 - y)
        return jnp.where(y == 0, z, back)

    def index(pos):
        q = jnp.maximum(pos - nz, 0)
        k, r = q // rest, q % rest
        odd = k % 2
        back = (nz - 1 - k) * ny + (1 - odd) * (1 + r) + odd * (ny - 1 - r)
        return jnp.where(pos < nz, pos * ny, back)

    return position, index


def kernel(
    n, n_tp, tokens_hbm, norm_gain, gate_hbm, up_hbm, down_hbm, out_gain, out_ref,
    tok, normed, gate, up, down, gate_acc, up_acc, hidden, parts, sib, far, own, sq, sq_all,
    local_sem, ring_send, ring_recv, sib_send, sib_recv, far_send, far_recv, sq_send, sq_recv,
):
    half = n // 2
    nx, cuts = n_tp // 2, down.shape[0] // n
    nb = n * cuts // n_tp
    n_tok, d_model = tok.shape
    rows_in = gate.shape[1]
    n_hid, width = down.shape[1], down.shape[2]
    piece = n_tok // PIECES
    position, index = ring_layout(n, n_tp)
    fs, tp = lax.axis_index("fs"), lax.axis_index("tp")
    x, core = tp // 2, tp % 2
    me = position(fs)
    block_of = {}
    for h in range(half + 1):
        block_of[0, h] = index((me + n - h) % n)
        block_of[1, h] = index((me + h) % n)
    target = (block_of[1, 1], block_of[0, 1])
    sibling = x * 2 + 1 - core

    barrier = pltpu.get_barrier_semaphore()
    for fs_id in target:
        pl.semaphore_signal(barrier, inc=1, device_id={"fs": fs_id}, device_id_type=MESH)
    for d in range(1, n_tp):
        pl.semaphore_signal(
            barrier, inc=1, device_id={"tp": (tp + d) % n_tp}, device_id_type=MESH
        )
    loads = [
        pltpu.make_async_copy(tokens_hbm, tok, local_sem.at[0]),
        pltpu.make_async_copy(gate_hbm, gate.at[fs], local_sem.at[1]),
        pltpu.make_async_copy(up_hbm, up.at[fs], local_sem.at[2]),
    ]
    for j in range(cuts):
        cols = pl.ds(j * width, width)
        loads.append(
            pltpu.make_async_copy(
                down_hbm.at[:, cols], down.at[fs * cuts + j], local_sem.at[3 + j]
            )
        )
    for load in loads:
        load.start()
    pl.semaphore_wait(barrier, 2 + n_tp - 1)

    def view(c, b, h, way):
        if c < 2:
            ref = (gate, up)[c]
            if h == half:
                return ref.at[b, pl.ds(way * (rows_in // 2), rows_in // 2)]
            return ref.at[b]
        if h == half:
            return down.at[b * cuts + c - 2, pl.ds(way * (n_hid // 2), n_hid // 2)]
        return down.at[b * cuts + c - 2]

    def ring_copy(c, way, h, b, first=False):
        dst = view(c, b, h, way)
        src = (gate_hbm, up_hbm)[c] if first and c < 2 else dst
        return pltpu.make_async_remote_copy(
            src_ref=src,
            dst_ref=dst,
            send_sem=ring_send.at[way, h - 1, c],
            recv_sem=ring_recv.at[way, h - 1, c],
            device_id={"fs": target[way]},
            device_id_type=MESH,
        )

    sends = []

    def send(c, way, h):
        copy = ring_copy(c, way, h, block_of[way, h - 1], h == 1)
        copy.start()
        sends.append(copy)

    def arrive(c, way, h):
        ring_copy(c, way, h, block_of[way, h]).wait_recv()

    for c in (0, 1):
        for way in (0, 1):
            send(c, way, 1)

    loads[0].wait()
    tile = min(128, n_tok)

    @pl.loop(0, n_tok // tile)
    def _(i):
        rows = pl.ds(pl.multiple_of(i * tile, tile), tile)
        v = tok[rows, :].astype(jnp.float32)
        r = lax.rsqrt(jnp.mean(v * v, axis=1, keepdims=True) + EPSILON)
        out = (v * r * norm_gain[...]).astype(jnp.bfloat16)
        for j in range(n):
            normed[j, rows, :] = out[:, j * rows_in:(j + 1) * rows_in]

    def accumulate(b, mode):
        n_col = gate.shape[2]
        step = min(COLUMN_TILE, n_col)

        @pl.loop(0, n_col // step)
        def _(i):
            cols = pl.ds(pl.multiple_of(i * step, step), step)
            a = normed[b]
            g = jnp.dot(a, gate[b, :, cols], preferred_element_type=jnp.float32)
            u = jnp.dot(a, up[b, :, cols], preferred_element_type=jnp.float32)
            if mode != "first":
                g = g + gate_acc[:, cols]
                u = u + up_acc[:, cols]
            if mode == "last":
                hidden[:, cols] = (g * (1.0 / (1.0 + jnp.exp(-g))) * u).astype(jnp.bfloat16)
            else:
                gate_acc[:, cols] = g
                up_acc[:, cols] = u

    loads[1].wait()
    loads[2].wait()
    accumulate(fs, "first")
    for load in loads[3:]:
        load.wait()

    for h in range(1, half + 1):
        for c in (0, 1):
            for way in (0, 1):
                arrive(c, way, h)
                if h < half:
                    send(c, way, h + 1)
        if h == half - 1:
            for j in range(cuts):
                for way in (0, 1):
                    send(2 + j, way, 1)
        if h < half:
            accumulate(block_of[0, h], "mid")
            accumulate(block_of[1, h], "mid")
        else:
            accumulate(block_of[0, h], "last")

    def owner(b):
        t = b // nb
        return t // 2, t % 2, b % nb

    def piece_rows(q):
        return pl.ds(pl.multiple_of(q * piece, piece), piece)

    def sib_copy(b, slot, q):
        return pltpu.make_async_remote_copy(
            src_ref=parts.at[b, piece_rows(q)],
            dst_ref=sib.at[slot, piece_rows(q)],
            send_sem=sib_send.at[slot, q],
            recv_sem=sib_recv.at[slot, q],
            device_id={"tp": sibling},
            device_id_type=MESH,
        )

    def far_copy(b, x_to, x_from, k, q):
        return pltpu.make_async_remote_copy(
            src_ref=parts.at[b, piece_rows(q)],
            dst_ref=far.at[x_from, k, piece_rows(q)],
            send_sem=far_send.at[x_to * nb + k, q],
            recv_sem=far_recv.at[x_from, k, q],
            device_id={"tp": x_to * 2 + core},
            device_id_type=MESH,
        )

    def multiply(b):
        x_to, core_to, k = owner(b)

        @pl.loop(0, PIECES)
        def _(q):
            rows = piece_rows(q)
            parts[b, rows, :] = jnp.dot(
                hidden[rows, :], down[b], preferred_element_type=jnp.float32
            ).astype(jnp.bfloat16)

            @pl.when(core_to != core)
            def _():
                sib_copy(b, x_to * nb + k, q).start()

    def reduce(b):
        x_to, core_to, k = owner(b)

        @pl.when((core_to == core) & (x_to != x))
        def _():
            @pl.loop(0, PIECES)
            def _(q):
                rows = piece_rows(q)
                slot = x_to * nb + k
                sib_copy(b, slot, q).wait_recv()
                parts[b, rows, :] = (
                    parts[b, rows, :].astype(jnp.float32) + sib[slot, rows, :].astype(jnp.float32)
                ).astype(jnp.bfloat16)
                far_copy(b, x_to, x, k, q).start()

    ready = [fs * cuts + j for j in range(cuts)]
    for h in range(1, half + 1):
        for j in range(cuts):
            for way in (0, 1):
                arrive(2 + j, way, h)
                if h < half:
                    send(2 + j, way, h + 1)
            for way in (0, 1) if h < half else (0,):
                ready.append(block_of[way, h] * cuts + j)
            for b in ready:
                multiply(b)
            for b in ready:
                reduce(b)
            ready = []

    @pl.loop(0, PIECES)
    def _(q):
        rows = piece_rows(q)
        squares = jnp.zeros((piece, 1), jnp.float32)
        for k in range(nb):
            b, slot = tp * nb + k, x * nb + k
            v = parts[b, rows, :].astype(jnp.float32)
            sib_copy(b, slot, q).wait_recv()
            v = v + sib[slot, rows, :].astype(jnp.float32)
            for d in range(1, nx):
                x_from = (x + d) % nx
                far_copy(b, x, x_from, k, q).wait_recv()
                v = v + far[x_from, k, rows, :].astype(jnp.float32)
            own[k, rows, :] = v
            squares = squares + jnp.sum(v * v, axis=1, keepdims=True)
        sq[q] = jnp.transpose(jnp.broadcast_to(squares, (piece, 128)))[0:8, :]

    def sq_copy(to, slot):
        return pltpu.make_async_remote_copy(
            src_ref=sq,
            dst_ref=sq_all.at[slot],
            send_sem=sq_send.at[to],
            recv_sem=sq_recv.at[slot],
            device_id={"tp": to},
            device_id_type=MESH,
        )

    others = [(tp + d) % n_tp for d in range(1, n_tp)]
    for t in others:
        sq_copy(t, tp).start()
    for t in others:
        sq_copy(t, t).wait_recv()

    @pl.loop(0, PIECES)
    def _(q):
        rows = piece_rows(q)
        total = sq[q]
        for t in others:
            total = total + sq_all[t, q]
        r = lax.rsqrt(total / d_model + EPSILON)
        r = jnp.transpose(jnp.broadcast_to(r[0:1, :], (128, piece)))[:, 0:1]
        for k in range(nb):
            cols = slice(k * width, (k + 1) * width)
            out_ref[rows, cols] = (own[k, rows, :] * r * out_gain[:, cols]).astype(jnp.bfloat16)

    for t in others:
        sq_copy(t, tp).wait_send()
    for copy in sends:
        copy.wait_send()

    @pl.loop(0, PIECES)
    def _(q):
        for slot in range(nx * nb):
            sib_copy(slot, slot, q).wait_send()
        for d in range(1, nx):
            for k in range(nb):
                far_copy(k, (x + d) % nx, x, k, q).wait_send()


def body(n, n_tp, tokens, norm_gain, gate_weight, up_weight, down_weight, out_gain):
    n_tok, d_model = tokens.shape
    rows_in, n_hid = gate_weight.shape
    cuts = max(down_weight.shape[1] // 128, 1)
    width = down_weight.shape[1] // cuts
    half, nx, nb = n // 2, n_tp // 2, n * cuts // n_tp
    piece = n_tok // PIECES
    bf16, f32 = jnp.bfloat16, jnp.float32
    dma = pltpu.SemaphoreType.DMA
    hbm = pl.BlockSpec(memory_space=pl.ANY)
    vmem = pl.BlockSpec(memory_space=pltpu.VMEM)
    return pl.pallas_call(
        functools.partial(kernel, n, n_tp),
        out_shape=jax.ShapeDtypeStruct((n_tok, out_gain.shape[0]), bf16),
        in_specs=[hbm, vmem, hbm, hbm, hbm, vmem],
        out_specs=vmem,
        scratch_shapes=[
            pltpu.VMEM((n_tok, d_model), bf16),
            pltpu.VMEM((n, n_tok, rows_in), bf16),
            pltpu.VMEM((n, rows_in, n_hid), bf16),
            pltpu.VMEM((n, rows_in, n_hid), bf16),
            pltpu.VMEM((n * cuts, n_hid, width), bf16),
            pltpu.VMEM((n_tok, n_hid), f32),
            pltpu.VMEM((n_tok, n_hid), f32),
            pltpu.VMEM((n_tok, n_hid), bf16),
            pltpu.VMEM((n * cuts, n_tok, width), bf16),
            pltpu.VMEM((nx * nb, n_tok, width), bf16),
            pltpu.VMEM((nx, nb, n_tok, width), bf16),
            pltpu.VMEM((nb, n_tok, width), f32),
            pltpu.VMEM((PIECES, 8, piece), f32),
            pltpu.VMEM((n_tp, PIECES, 8, piece), f32),
            dma((3 + cuts,)),
            dma((2, half, 2 + cuts)),
            dma((2, half, 2 + cuts)),
            dma((nx * nb, PIECES)),
            dma((nx * nb, PIECES)),
            dma((nx * nb, PIECES)),
            dma((nx, nb, PIECES)),
            dma((n_tp,)),
            dma((n_tp,)),
        ],
        compiler_params=pltpu.CompilerParams(
            collective_id=0, has_side_effects=True, vmem_limit_bytes=62 * 1024 * 1024
        ),
        name="ffn_ring",
    )(tokens, norm_gain[None, :], gate_weight, up_weight, down_weight, out_gain[None, :])


def line_order(k, nz):
    others = [s for s in range(nz) if s != k]
    return sorted(others, key=lambda s: (abs(s - k), abs(2 * s - nz + 1)))


def inward_order(k, nz):
    out = line_order(k, nz)
    if k in (0, nz - 1):
        out = out[1:] + out[:1]
    return out


def line_kernel(
    n, n_tp, tokens_hbm, norm_gain, gate_hbm, up_hbm, down_hbm, out_gain, out_hbm,
    result, tok, normed, gate, up, down, gate_acc, up_acc, hidden, parts, sib, near, far, own, squares, sq, sq_all,
    local_sem, y_send, y_recv, z_send, z_recv, tok_send, tok_recv,
    sib_send, sib_recv, near_send, near_recv, far_send, far_recv, sq_send, sq_recv, out_sem,
):
    nz = n // 2
    cuts = down.shape[0] // n
    nb = n * cuts // n_tp
    n_own, d_model = tok.shape
    rows_in, n_hid = gate.shape[1], gate.shape[2]
    width = down.shape[2]
    quarter = n_own // n_tp
    small = quarter // TOKEN_PIECES
    half_rows = n_own // PIECES
    fs, tp = lax.axis_index("fs"), lax.axis_index("tp")
    z, y = fs // 2, fs % 2
    x, core = tp // 2, tp % 2
    fs_y = z * 2 + 1 - y
    sibling, across = x * 2 + 1 - core, (1 - x) * 2 + core
    has_next = (z < nz - 1, z > 0)
    inner = (z > 0) & (z < nz - 1)
    outer = jnp.logical_not(inner)
    inward = jnp.where(z < nz // 2, 0, 1)

    barrier = pltpu.get_barrier_semaphore()
    pl.semaphore_signal(barrier, inc=1, device_id={"fs": fs_y}, device_id_type=MESH)
    for d in range(1, n_tp):
        pl.semaphore_signal(
            barrier, inc=1, device_id={"tp": (tp + d) % n_tp}, device_id_type=MESH
        )
    for way in (0, 1):

        @pl.when(has_next[way])
        def _():
            to = {"fs": fs + 2 - 4 * way}
            pl.semaphore_signal(barrier, inc=1, device_id=to, device_id_type=MESH)

    keep = pl.ds(pl.multiple_of(y * n_hid, n_hid), n_hid)
    give = pl.ds(pl.multiple_of((1 - y) * n_hid, n_hid), n_hid)
    loads = [
        pltpu.make_async_copy(tokens_hbm, tok, local_sem.at[0]),
        pltpu.make_async_copy(gate_hbm.at[:, keep], gate.at[fs], local_sem.at[1]),
        pltpu.make_async_copy(up_hbm.at[:, keep], up.at[fs], local_sem.at[2]),
    ]
    for j in range(cuts):
        cols = pl.ds(j * width, width)
        loads.append(
            pltpu.make_async_copy(
                down_hbm.at[keep, cols], down.at[fs * cuts + j], local_sem.at[3 + j]
            )
        )
    for load in loads:
        load.start()
    pl.semaphore_wait(barrier, n_tp + (z > 0).astype(jnp.int32) + (z < nz - 1).astype(jnp.int32))

    def shard(layer, other):
        return layer * 2 + (1 - y if other else y)

    def view(p, layer):
        if p < 4:
            return (gate, up)[p % 2].at[shard(layer, p // 2)]
        j = p - 4
        return down.at[layer * 2 * cuts + j]

    def z_copy(p, way, h, layer, src=None):
        dst = view(p, layer)
        return pltpu.make_async_remote_copy(
            src_ref=dst if src is None else src,
            dst_ref=dst,
            send_sem=z_send.at[way, h - 1, p],
            recv_sem=z_recv.at[way, h - 1, p],
            device_id={"fs": fs + 2 - 4 * way},
            device_id_type=MESH,
        )

    def send_own(p, where=None):
        src = (gate_hbm, up_hbm)[p].at[:, keep] if p < 2 else None
        for way in (0, 1):

            @pl.when(has_next[way] if where is None else has_next[way] & where(way))
            def _():
                z_copy(p, way, 1, z, src).start()

    order = [line_order(k, nz) for k in range(nz)]

    def pick(values):
        out = jnp.int32(values[0])
        for k in range(1, nz):
            out = jnp.where(z == k, values[k], out)
        return out

    sources = []
    for i in range(nz - 1):
        layer = pick([order[k][i] for k in range(nz)])
        way = pick([int(order[k][i] > k) for k in range(nz)])
        h = pick([abs(order[k][i] - k) for k in range(nz)])
        onward = pick([int(0 < k < nz - 1) for k in range(nz)]) == 1
        sources.append((layer, way, h, onward))

    def receive(i, p):
        layer, way, h, onward = sources[i]
        z_copy(p, way, h, layer).wait_recv()

        @pl.when(onward)
        def _():
            z_copy(p, way, h + 1, layer).start()

    def take(j):
        for i in range(nz - 1):
            if i != 1:
                receive(i, 4 + j)
        send_own(4 + j, lambda way: inward != way)

    def y_copy(p):
        if p < 2:
            src, dst = (gate_hbm, up_hbm)[p].at[:, give], (gate, up)[p]
            src, got = src, (gate, up)[p].at[fs_y]
            dst = (gate, up)[p].at[fs]
        elif p < 2 + cuts:
            j = p - 2
            src = down_hbm.at[give, pl.ds(j * width, width)]
            dst = down.at[fs * cuts + j]
        else:
            rows = token_rows(y, tp, p - 2 - cuts)
            src = dst = normed.at[:, rows]
        return pltpu.make_async_remote_copy(
            src_ref=src,
            dst_ref=dst,
            send_sem=y_send.at[p],
            recv_sem=y_recv.at[p],
            device_id={"fs": fs_y},
            device_id_type=MESH,
        )

    def token_rows(y_of, t, p):
        start = y_of * n_own + t * quarter + p * small
        return pl.ds(pl.multiple_of(start, small), small)

    def token_copy(kind, t, p, to):
        part = normed.at[:, token_rows(1 - y, t, p)]
        return pltpu.make_async_remote_copy(
            src_ref=part,
            dst_ref=part,
            send_sem=tok_send.at[kind, p],
            recv_sem=tok_recv.at[kind, p],
            device_id={"tp": to},
            device_id_type=MESH,
        )

    for p in (0, 1):
        send_own(p)
    for p in (0, 1):
        y_copy(p).start()

    loads[0].wait()
    tile = min(128, n_own)
    tiles = n_own // tile
    own_tiles = quarter // tile

    def normalize(i):
        rows = pl.ds(pl.multiple_of(i * tile, tile), tile)
        rows_to = pl.ds(pl.multiple_of(y * n_own + i * tile, tile), tile)
        v = tok[rows, :].astype(jnp.float32)
        r = lax.rsqrt(jnp.mean(v * v, axis=1, keepdims=True) + EPSILON)
        out = (v * r * norm_gain[...]).astype(jnp.bfloat16)
        for j in range(n):
            normed[j, rows_to, :] = out[:, j * rows_in:(j + 1) * rows_in]

    @pl.loop(0, own_tiles)
    def _(i):
        normalize(tp * own_tiles + i)

    for p in range(TOKEN_PIECES):
        y_copy(2 + cuts + p).start()
    for j in range(cuts):
        y_copy(2 + j).start()

    def accumulate(c, b, y_of, mode="mid"):
        weight, acc = (gate, up)[c], (gate_acc, up_acc)[c]
        step = min(COLUMN_TILE, n_hid)
        n_col = n_hid // step

        def part(half, i):
            rows = pl.ds(pl.multiple_of(half * n_own, n_own), n_own)
            cols = pl.ds(pl.multiple_of(i * step, step), step)
            v = jnp.dot(normed[b, rows, :], weight[b, :, cols], preferred_element_type=jnp.float32)
            if mode != "first":
                v = v + acc[rows, cols]
            if mode == "last":
                g = gate_acc[rows, cols]
                hidden[rows, cols] = (g * (1.0 / (1.0 + jnp.exp(-g))) * v).astype(jnp.bfloat16)
            else:
                acc[rows, cols] = v

        @pl.loop(0, n_col if y_of is not None else 2 * n_col)
        def _(i):
            part(*((y_of, i) if y_of is not None else (i // n_col, i % n_col)))

    def tokens_in(p):
        y_copy(2 + cuts + p).wait_recv()
        token_copy(0, tp, p, across).start()
        token_copy(1, tp, p, sibling).start()

    def tokens_on(p):
        token_copy(0, across, p, across).wait_recv()
        token_copy(2, across, p, sibling).start()

    @pl.loop(own_tiles, tiles // 2)
    def _(i):
        normalize((tp * own_tiles + i) % tiles)

    y_copy(0).wait_recv()
    send_own(2)

    @pl.loop(tiles // 2, tiles)
    def _(i):
        normalize((tp * own_tiles + i) % tiles)

    for load in loads[1:]:
        load.wait()
    y_copy(1).wait_recv()
    send_own(3)
    for p in (0, 1):
        receive(0, p)
    for c in (0, 1):
        accumulate(c, fs, y, "first")
    for p in range(TOKEN_PIECES // 2):
        tokens_in(p)
    for c in (0, 1):
        accumulate(c, fs_y, y)
    for p in (2, 3):
        receive(0, p)

    @pl.when(inner)
    def _():
        for i in range(1, nz - 2):
            for p in range(4):
                receive(i, p)

    for p in range(TOKEN_PIECES // 2, TOKEN_PIECES):
        tokens_in(p)
        tokens_on(p - TOKEN_PIECES // 2)
    for p in (0, 1):
        accumulate(p, shard(sources[0][0], 0), y)
    for j in range(cuts):
        y_copy(2 + j).wait_recv()
    for j in range(2 * cuts):
        send_own(4 + j, lambda way: outer)
    for j in range(2 * cuts):
        send_own(4 + j, lambda way: inner & (inward == way))
    for p in range(TOKEN_PIECES // 2, TOKEN_PIECES):
        tokens_on(p)
    for p in (0, 1):
        accumulate(p, shard(sources[0][0], 1), y)

    @pl.when(outer)
    def _():
        for i in range(1, nz - 2):
            for p in range(4):
                receive(i, p)

    for p in range(TOKEN_PIECES):
        token_copy(1, sibling, p, sibling).wait_recv()
        token_copy(2, across + 1 - 2 * core, p, sibling).wait_recv()

    last = nz - 2

    def receive_if(where, p):
        @pl.when(where)
        def _():
            receive(last, p)

    for p in range(3):
        receive_if(inner, p)

    for c in (0, 1):
        accumulate(c, fs, 1 - y, "first")
        accumulate(c, fs_y, 1 - y)
        for p in (0, 1):
            accumulate(c, shard(sources[0][0], p), 1 - y)
    receive_if(inner, 3)
    for i in range(1, nz - 2):
        for p in (0, 1):
            accumulate(p, shard(sources[i][0], 0), None)
    for i in range(1, nz - 2):
        for p in (0, 1):
            accumulate(p, shard(sources[i][0], 1), None)

    @pl.when(inner)
    def _():
        for j in range(2 * cuts):
            receive(1, 4 + j)

    receive_if(outer, 0)
    accumulate(0, shard(sources[last][0], 0), None)
    receive_if(outer, 1)
    accumulate(1, shard(sources[last][0], 0), None)
    receive_if(outer, 2)
    accumulate(0, shard(sources[last][0], 1), None)
    receive_if(outer, 3)

    accumulate(1, shard(sources[last][0], 1), None, "last")

    def owner(b):
        t = b // nb
        return t // 2, t % 2, b % nb

    def block_rows(q):
        return pl.ds(pl.multiple_of(q * n_own, n_own), n_own)

    def sib_copy(b, slot, q):
        return pltpu.make_async_remote_copy(
            src_ref=parts.at[b, block_rows(q)],
            dst_ref=sib.at[slot, block_rows(q)],
            send_sem=sib_send.at[slot, q],
            recv_sem=sib_recv.at[slot, q],
            device_id={"tp": sibling},
            device_id_type=MESH,
        )

    def part_rows(q, r):
        return pl.ds(pl.multiple_of(q * n_own + r * half_rows, half_rows), half_rows)

    def near_copy(b, q, r, slot, to):
        return pltpu.make_async_remote_copy(
            src_ref=parts.at[b, part_rows(q, r)],
            dst_ref=near.at[slot, part_rows(0, r)],
            send_sem=near_send.at[slot, r],
            recv_sem=near_recv.at[slot, r],
            device_id=to,
            device_id_type=MESH,
        )

    def far_copy(b, q, r, k, sent, to):
        return pltpu.make_async_remote_copy(
            src_ref=parts.at[b, part_rows(q, r)],
            dst_ref=far.at[k, part_rows(0, r)],
            send_sem=far_send.at[sent, r],
            recv_sem=far_recv.at[k, r],
            device_id=to,
            device_id_type=MESH,
        )

    to_y, to_x = {"fs": fs_y}, {"tp": across}

    def multiply(b):
        x_to, core_to, k = owner(b)

        @pl.loop(0, 2)
        def _(q):
            rows = block_rows(q)
            parts[b, rows, :] = jnp.dot(
                hidden[rows, :], down[b], preferred_element_type=jnp.float32
            ).astype(jnp.bfloat16)

            @pl.when(core_to != core)
            def _():
                sib_copy(b, x_to * nb + k, q).start()

    def fold(b, slot, q, r, extra=None):
        rows = part_rows(q, r)
        v = parts[b, rows, :].astype(jnp.float32) + sib[slot, rows, :].astype(jnp.float32)
        if extra is not None:
            v = v + near[extra, part_rows(0, r), :].astype(jnp.float32)
        parts[b, rows, :] = v.astype(jnp.bfloat16)

    def starts_on_y(x_to, core_to, k):
        same = x_to == z // (nz // 2)
        own_layer = x_to * 2 + core_to == z
        return (k + x_to + core_to) % 2 == 1

    def near_slot(y_first, x_to, k, q):
        return jnp.where(y_first, x_to, 2 + q) * nb + k

    def reduce(b):
        x_to, core_to, k = owner(b)
        y_first = starts_on_y(x_to, core_to, k)
        slot = x_to * nb + k

        @pl.when((core_to == core) & (y_first | (x_to != x)))
        def _():
            q = 1 - y
            to = {"fs": jnp.where(y_first, fs_y, fs), "tp": jnp.where(y_first, tp, across)}
            sib_copy(b, slot, q).wait_recv()
            for r in range(PIECES):
                fold(b, slot, q, r)
                near_copy(b, q, r, near_slot(y_first, x_to, k, q), to).start()

            @pl.when(jnp.logical_not(y_first))
            def _():
                sib_copy(b, slot, y).wait_recv()
                for r in range(PIECES):
                    fold(b, slot, y, r)
                    near_copy(b, y, r, near_slot(False, x_to, k, y), to_x).start()

    def pass_on(b):
        x_to, core_to, k = owner(b)
        y_first = starts_on_y(x_to, core_to, k)
        slot = x_to * nb + k

        @pl.when((core_to == core) & (y_first == (x_to != x)))
        def _():
            q = jnp.where(y_first, y, 1 - y)
            got = near_slot(y_first, x_to, k, q)
            to = {"fs": jnp.where(y_first, fs, fs_y), "tp": jnp.where(y_first, across, tp)}
            sib_copy(b, slot, q).wait_recv()
            for r in range(PIECES):
                near_copy(b, q, r, got, to_y).wait_recv()
                fold(b, slot, q, r, got)
                far_copy(b, q, r, k, slot, to).start()

    final_order = [[k] + inward_order(k, nz) for k in range(nz)]
    steps = []

    def run(b):
        m = len(steps)
        steps.append(b)
        multiply(b)
        if m >= 1:
            reduce(steps[m - 1])
        if m >= LAG:
            pass_on(steps[m - LAG])

    for j in range(2 * cuts):
        run(z * 2 * cuts + j)
    for j in range(2 * cuts):

        @pl.when(inner)
        def _():
            if j == 0:
                take(0)
            if j + 1 < 2 * cuts:
                take(j + 1)

        for i in range(1, nz):
            layer = pick([final_order[k][i] for k in range(nz)])
            way = pick([int(final_order[k][i] > k) for k in range(nz)])
            h = pick([abs(final_order[k][i] - k) for k in range(nz)])

            @pl.when(outer)
            def _():
                z_copy(4 + j, way, h, layer).wait_recv()

            run(layer * 2 * cuts + j)
    reduce(steps[-1])
    for b in steps[-LAG:]:
        pass_on(b)

    def piece_rows(q):
        return pl.ds(pl.multiple_of(q * half_rows, half_rows), half_rows)

    def out_copy(q):
        rows = piece_rows(q)
        return pltpu.make_async_copy(result.at[rows], out_hbm.at[rows], out_sem.at[q])

    for k in range(nb):
        slot = near_slot(starts_on_y(x, core, k), x, k, y)
        sib_copy(0, x * nb + k, y).wait_recv()
        for r in range(PIECES):
            near_copy(0, 0, r, slot, to_x).wait_recv()
        for r in range(PIECES):
            far_copy(0, 0, r, k, k, to_x).wait_recv()

        @pl.loop(0, n_own // tile)
        def _(i):
            rows = pl.ds(pl.multiple_of(i * tile, tile), tile)
            mine = pl.ds(pl.multiple_of(y * n_own + i * tile, tile), tile)
            v = parts[tp * nb + k, mine, :].astype(jnp.float32)
            v = v + sib[x * nb + k, mine, :].astype(jnp.float32)
            v = v + near[slot, rows, :].astype(jnp.float32)
            v = v + far[k, rows, :].astype(jnp.float32)
            own[k, rows, :] = v
            squares[rows, :] = v * v if k == 0 else squares[rows, :] + v * v

    for q in range(PIECES):
        total = jnp.sum(squares[piece_rows(q), :], axis=1, keepdims=True)
        sq[q] = jnp.transpose(jnp.broadcast_to(total, (half_rows, 128)))[0:8, :]

    def sq_copy(to, slot):
        return pltpu.make_async_remote_copy(
            src_ref=sq,
            dst_ref=sq_all.at[slot],
            send_sem=sq_send.at[to],
            recv_sem=sq_recv.at[slot],
            device_id={"tp": to},
            device_id_type=MESH,
        )

    others = [(tp + d) % n_tp for d in range(1, n_tp)]
    for t in others:
        sq_copy(t, tp).start()
    for p in range(2 + cuts + TOKEN_PIECES):
        y_copy(p).wait_send()
    for p in range(TOKEN_PIECES):
        token_copy(0, tp, p, across).wait_send()
        token_copy(1, tp, p, sibling).wait_send()
        token_copy(2, across, p, sibling).wait_send()
    for p in range(4 + 2 * cuts):
        for way in (0, 1):

            @pl.when(has_next[way])
            def _():
                z_copy(p, way, 1, z).wait_send()

        for layer, way, h, onward in sources:

            @pl.when(onward)
            def _():
                z_copy(p, way, h + 1, layer).wait_send()

    @pl.loop(0, 2)
    def _(q):
        for x_to in (0, 1):
            for k in range(nb):
                sib_copy(0, x_to * nb + k, q).wait_send()

    for x_to in (0, 1):
        for k in range(nb):
            y_first = starts_on_y(x_to, core, k)

            @pl.when(y_first)
            def _():
                for r in range(PIECES):
                    near_copy(0, 0, r, near_slot(True, x_to, k, 0), to_x).wait_send()

            @pl.when(jnp.logical_not(y_first) & (x_to != x))
            def _():
                for q in (0, 1):
                    for r in range(PIECES):
                        near_copy(0, 0, r, near_slot(False, x_to, k, q), to_x).wait_send()

            @pl.when(y_first == (x_to != x))
            def _():
                for r in range(PIECES):
                    far_copy(0, 0, r, k, x_to * nb + k, to_x).wait_send()

    for t in others:
        sq_copy(t, t).wait_recv()

    for q in range(PIECES):
        rows = piece_rows(q)
        total = sq[q]
        for t in others:
            total = total + sq_all[t, q]
        r = lax.rsqrt(total / d_model + EPSILON)
        r = jnp.transpose(jnp.broadcast_to(r[0:1, :], (128, half_rows)))
        for k in range(nb):
            cols = slice(k * width, (k + 1) * width)
            result[rows, cols] = (own[k, rows, :] * r * out_gain[:, cols]).astype(jnp.bfloat16)
        out_copy(q).start()
    for q in range(PIECES):
        out_copy(q).wait()

    for t in others:
        sq_copy(t, tp).wait_send()


def line_body(n, n_tp, tokens, norm_gain, gate_weight, up_weight, down_weight, out_gain):
    n_own, d_model = tokens.shape
    rows_in, n_hid = gate_weight.shape[0], gate_weight.shape[1] // 2
    cuts = max(down_weight.shape[1] // 128, 1)
    width = down_weight.shape[1] // cuts
    nz, nb = n // 2, n * cuts // n_tp
    n_tok = 2 * n_own
    bf16, f32 = jnp.bfloat16, jnp.float32
    dma = pltpu.SemaphoreType.DMA
    hbm = pl.BlockSpec(memory_space=pl.ANY)
    vmem = pl.BlockSpec(memory_space=pltpu.VMEM)
    return pl.pallas_call(
        functools.partial(line_kernel, n, n_tp),
        out_shape=jax.ShapeDtypeStruct((n_own, out_gain.shape[0]), bf16),
        in_specs=[hbm, vmem, hbm, hbm, hbm, vmem],
        out_specs=hbm,
        scratch_shapes=[
            pltpu.VMEM((n_own, out_gain.shape[0]), bf16),
            pltpu.VMEM((n_own, d_model), bf16),
            pltpu.VMEM((n, n_tok, rows_in), bf16),
            pltpu.VMEM((n, rows_in, n_hid), bf16),
            pltpu.VMEM((n, rows_in, n_hid), bf16),
            pltpu.VMEM((n * cuts, n_hid, width), bf16),
            pltpu.VMEM((n_tok, n_hid), f32),
            pltpu.VMEM((n_tok, n_hid), f32),
            pltpu.VMEM((n_tok, n_hid), bf16),
            pltpu.VMEM((n * cuts, n_tok, width), bf16),
            pltpu.VMEM((2 * nb, n_tok, width), bf16),
            pltpu.VMEM((4 * nb, n_own, width), bf16),
            pltpu.VMEM((nb, n_own, width), bf16),
            pltpu.VMEM((nb, n_own, width), f32),
            pltpu.VMEM((n_own, width), f32),
            pltpu.VMEM((PIECES, 8, n_own // PIECES), f32),
            pltpu.VMEM((n_tp, PIECES, 8, n_own // PIECES), f32),
            dma((3 + cuts,)),
            dma((2 + cuts + TOKEN_PIECES,)),
            dma((2 + cuts + TOKEN_PIECES,)),
            dma((2, nz - 1, 4 + 2 * cuts)),
            dma((2, nz - 1, 4 + 2 * cuts)),
            dma((3, TOKEN_PIECES)),
            dma((3, TOKEN_PIECES)),
            dma((2 * nb, 2)),
            dma((2 * nb, 2)),
            dma((4 * nb, PIECES)),
            dma((4 * nb, PIECES)),
            dma((2 * nb, PIECES)),
            dma((nb, PIECES)),
            dma((n_tp,)),
            dma((n_tp,)),
            dma((PIECES,)),
        ],
        compiler_params=pltpu.CompilerParams(
            collective_id=0, has_side_effects=True, vmem_limit_bytes=62 * 1024 * 1024
        ),
        name="ffn_line",
    )(tokens, norm_gain[None, :], gate_weight, up_weight, down_weight, out_gain[None, :])


def solution(mesh):
    n, n_tp = mesh.shape["fs"], mesh.shape["tp"]
    paired = n_tp == 4 and n % 2 == 0 and n // 2 > 2
    return jax.shard_map(
        functools.partial(line_body if paired else body, n, n_tp),
        mesh=mesh,
        in_specs=(P("fs", None), P(), P("fs", "tp"), P("fs", "tp"), P("tp", "fs"), P("tp")),
        out_specs=P("fs", "tp"),
        check_vma=False,
    )
```

```python
import functools

import jax
import jax.numpy as jnp
from jax import lax
from jax.experimental import pallas as pl
from jax.experimental.pallas import tpu as pltpu
from jax.sharding import PartitionSpec as P

EPSILON = 1e-06
MESH = pl.DeviceIdType.MESH
PIECES = 2
COLUMN_TILE = 256
TOKEN_PIECES = 4
LAG = 5
FIRST = 2


def ring_layout(n, n_tp):
    ny = max(n_tp // 2, 1)
    if n % ny or (n // ny) % 2:
        ny = 1
    nz, rest = n // ny, max(ny - 1, 1)

    def position(fs):
        z, y = fs // ny, fs % ny
        k = nz - 1 - z
        odd = k % 2
        back = nz + k * rest + (1 - odd) * (y - 1) + odd * (ny - 1 - y)
        return jnp.where(y == 0, z, back)

    def index(pos):
        q = jnp.maximum(pos - nz, 0)
        k, r = q // rest, q % rest
        odd = k % 2
        back = (nz - 1 - k) * ny + (1 - odd) * (1 + r) + odd * (ny - 1 - r)
        return jnp.where(pos < nz, pos * ny, back)

    return position, index


def kernel(
    n, n_tp, tokens_hbm, norm_gain, gate_hbm, up_hbm, down_hbm, out_gain, out_ref,
    tok, normed, gate, up, down, gate_acc, up_acc, hidden, parts, sib, far, own, sq, sq_all,
    local_sem, ring_send, ring_recv, sib_send, sib_recv, far_send, far_recv, sq_send, sq_recv,
):
    half = n // 2
    nx, cuts = n_tp // 2, down.shape[0] // n
    nb = n * cuts // n_tp
    n_tok, d_model = tok.shape
    rows_in = gate.shape[1]
    n_hid, width = down.shape[1], down.shape[2]
    piece = n_tok // PIECES
    position, index = ring_layout(n, n_tp)
    fs, tp = lax.axis_index("fs"), lax.axis_index("tp")
    x, core = tp // 2, tp % 2
    me = position(fs)
    block_of = {}
    for h in range(half + 1):
        block_of[0, h] = index((me + n - h) % n)
        block_of[1, h] = index((me + h) % n)
    target = (block_of[1, 1], block_of[0, 1])
    sibling = x * 2 + 1 - core

    barrier = pltpu.get_barrier_semaphore()
    for fs_id in target:
        pl.semaphore_signal(barrier, inc=1, device_id={"fs": fs_id}, device_id_type=MESH)
    for d in range(1, n_tp):
        pl.semaphore_signal(
            barrier, inc=1, device_id={"tp": (tp + d) % n_tp}, device_id_type=MESH
        )
    loads = [
        pltpu.make_async_copy(tokens_hbm, tok, local_sem.at[0]),
        pltpu.make_async_copy(gate_hbm, gate.at[fs], local_sem.at[1]),
        pltpu.make_async_copy(up_hbm, up.at[fs], local_sem.at[2]),
    ]
    for j in range(cuts):
        cols = pl.ds(j * width, width)
        loads.append(
            pltpu.make_async_copy(
                down_hbm.at[:, cols], down.at[fs * cuts + j], local_sem.at[3 + j]
            )
        )
    for load in loads:
        load.start()
    pl.semaphore_wait(barrier, 2 + n_tp - 1)

    def view(c, b, h, way):
        if c < 2:
            ref = (gate, up)[c]
            if h == half:
                return ref.at[b, pl.ds(way * (rows_in // 2), rows_in // 2)]
            return ref.at[b]
        if h == half:
            return down.at[b * cuts + c - 2, pl.ds(way * (n_hid // 2), n_hid // 2)]
        return down.at[b * cuts + c - 2]

    def ring_copy(c, way, h, b, first=False):
        dst = view(c, b, h, way)
        src = (gate_hbm, up_hbm)[c] if first and c < 2 else dst
        return pltpu.make_async_remote_copy(
            src_ref=src,
            dst_ref=dst,
            send_sem=ring_send.at[way, h - 1, c],
            recv_sem=ring_recv.at[way, h - 1, c],
            device_id={"fs": target[way]},
            device_id_type=MESH,
        )

    sends = []

    def send(c, way, h):
        copy = ring_copy(c, way, h, block_of[way, h - 1], h == 1)
        copy.start()
        sends.append(copy)

    def arrive(c, way, h):
        ring_copy(c, way, h, block_of[way, h]).wait_recv()

    for c in (0, 1):
        for way in (0, 1):
            send(c, way, 1)

    loads[0].wait()
    tile = min(128, n_tok)

    @pl.loop(0, n_tok // tile)
    def _(i):
        rows = pl.ds(pl.multiple_of(i * tile, tile), tile)
        v = tok[rows, :].astype(jnp.float32)
        r = lax.rsqrt(jnp.mean(v * v, axis=1, keepdims=True) + EPSILON)
        out = (v * r * norm_gain[...]).astype(jnp.bfloat16)
        for j in range(n):
            normed[j, rows, :] = out[:, j * rows_in:(j + 1) * rows_in]

    def accumulate(b, mode):
        n_col = gate.shape[2]
        step = min(COLUMN_TILE, n_col)

        @pl.loop(0, n_col // step)
        def _(i):
            cols = pl.ds(pl.multiple_of(i * step, step), step)
            a = normed[b]
            g = jnp.dot(a, gate[b, :, cols], preferred_element_type=jnp.float32)
            u = jnp.dot(a, up[b, :, cols], preferred_element_type=jnp.float32)
            if mode != "first":
                g = g + gate_acc[:, cols]
                u = u + up_acc[:, cols]
            if mode == "last":
                hidden[:, cols] = (g * (1.0 / (1.0 + jnp.exp(-g))) * u).astype(jnp.bfloat16)
            else:
                gate_acc[:, cols] = g
                up_acc[:, cols] = u

    loads[1].wait()
    loads[2].wait()
    accumulate(fs, "first")
    for load in loads[3:]:
        load.wait()

    for h in range(1, half + 1):
        for c in (0, 1):
            for way in (0, 1):
                arrive(c, way, h)
                if h < half:
                    send(c, way, h + 1)
        if h == half - 1:
            for j in range(cuts):
                for way in (0, 1):
                    send(2 + j, way, 1)
        if h < half:
            accumulate(block_of[0, h], "mid")
            accumulate(block_of[1, h], "mid")
        else:
            accumulate(block_of[0, h], "last")

    def owner(b):
        t = b // nb
        return t // 2, t % 2, b % nb

    def piece_rows(q):
        return pl.ds(pl.multiple_of(q * piece, piece), piece)

    def sib_copy(b, slot, q):
        return pltpu.make_async_remote_copy(
            src_ref=parts.at[b, piece_rows(q)],
            dst_ref=sib.at[slot, piece_rows(q)],
            send_sem=sib_send.at[slot, q],
            recv_sem=sib_recv.at[slot, q],
            device_id={"tp": sibling},
            device_id_type=MESH,
        )

    def far_copy(b, x_to, x_from, k, q):
        return pltpu.make_async_remote_copy(
            src_ref=parts.at[b, piece_rows(q)],
            dst_ref=far.at[x_from, k, piece_rows(q)],
            send_sem=far_send.at[x_to * nb + k, q],
            recv_sem=far_recv.at[x_from, k, q],
            device_id={"tp": x_to * 2 + core},
            device_id_type=MESH,
        )

    def multiply(b):
        x_to, core_to, k = owner(b)

        @pl.loop(0, PIECES)
        def _(q):
            rows = piece_rows(q)
            parts[b, rows, :] = jnp.dot(
                hidden[rows, :], down[b], preferred_element_type=jnp.float32
            ).astype(jnp.bfloat16)

            @pl.when(core_to != core)
            def _():
                sib_copy(b, x_to * nb + k, q).start()

    def reduce(b):
        x_to, core_to, k = owner(b)

        @pl.when((core_to == core) & (x_to != x))
        def _():
            @pl.loop(0, PIECES)
            def _(q):
                rows = piece_rows(q)
                slot = x_to * nb + k
                sib_copy(b, slot, q).wait_recv()
                parts[b, rows, :] = (
                    parts[b, rows, :].astype(jnp.float32) + sib[slot, rows, :].astype(jnp.float32)
                ).astype(jnp.bfloat16)
                far_copy(b, x_to, x, k, q).start()

    ready = [fs * cuts + j for j in range(cuts)]
    for h in range(1, half + 1):
        for j in range(cuts):
            for way in (0, 1):
                arrive(2 + j, way, h)
                if h < half:
                    send(2 + j, way, h + 1)
            for way in (0, 1) if h < half else (0,):
                ready.append(block_of[way, h] * cuts + j)
            for b in ready:
                multiply(b)
            for b in ready:
                reduce(b)
            ready = []

    @pl.loop(0, PIECES)
    def _(q):
        rows = piece_rows(q)
        squares = jnp.zeros((piece, 1), jnp.float32)
        for k in range(nb):
            b, slot = tp * nb + k, x * nb + k
            v = parts[b, rows, :].astype(jnp.float32)
            sib_copy(b, slot, q).wait_recv()
            v = v + sib[slot, rows, :].astype(jnp.float32)
            for d in range(1, nx):
                x_from = (x + d) % nx
                far_copy(b, x, x_from, k, q).wait_recv()
                v = v + far[x_from, k, rows, :].astype(jnp.float32)
            own[k, rows, :] = v
            squares = squares + jnp.sum(v * v, axis=1, keepdims=True)
        sq[q] = jnp.transpose(jnp.broadcast_to(squares, (piece, 128)))[0:8, :]

    def sq_copy(to, slot):
        return pltpu.make_async_remote_copy(
            src_ref=sq,
            dst_ref=sq_all.at[slot],
            send_sem=sq_send.at[to],
            recv_sem=sq_recv.at[slot],
            device_id={"tp": to},
            device_id_type=MESH,
        )

    others = [(tp + d) % n_tp for d in range(1, n_tp)]
    for t in others:
        sq_copy(t, tp).start()
    for t in others:
        sq_copy(t, t).wait_recv()

    @pl.loop(0, PIECES)
    def _(q):
        rows = piece_rows(q)
        total = sq[q]
        for t in others:
            total = total + sq_all[t, q]
        r = lax.rsqrt(total / d_model + EPSILON)
        r = jnp.transpose(jnp.broadcast_to(r[0:1, :], (128, piece)))[:, 0:1]
        for k in range(nb):
            cols = slice(k * width, (k + 1) * width)
            out_ref[rows, cols] = (own[k, rows, :] * r * out_gain[:, cols]).astype(jnp.bfloat16)

    for t in others:
        sq_copy(t, tp).wait_send()
    for copy in sends:
        copy.wait_send()

    @pl.loop(0, PIECES)
    def _(q):
        for slot in range(nx * nb):
            sib_copy(slot, slot, q).wait_send()
        for d in range(1, nx):
            for k in range(nb):
                far_copy(k, (x + d) % nx, x, k, q).wait_send()


def body(n, n_tp, tokens, norm_gain, gate_weight, up_weight, down_weight, out_gain):
    n_tok, d_model = tokens.shape
    rows_in, n_hid = gate_weight.shape
    cuts = max(down_weight.shape[1] // 128, 1)
    width = down_weight.shape[1] // cuts
    half, nx, nb = n // 2, n_tp // 2, n * cuts // n_tp
    piece = n_tok // PIECES
    bf16, f32 = jnp.bfloat16, jnp.float32
    dma = pltpu.SemaphoreType.DMA
    hbm = pl.BlockSpec(memory_space=pl.ANY)
    vmem = pl.BlockSpec(memory_space=pltpu.VMEM)
    return pl.pallas_call(
        functools.partial(kernel, n, n_tp),
        out_shape=jax.ShapeDtypeStruct((n_tok, out_gain.shape[0]), bf16),
        in_specs=[hbm, vmem, hbm, hbm, hbm, vmem],
        out_specs=vmem,
        scratch_shapes=[
            pltpu.VMEM((n_tok, d_model), bf16),
            pltpu.VMEM((n, n_tok, rows_in), bf16),
            pltpu.VMEM((n, rows_in, n_hid), bf16),
            pltpu.VMEM((n, rows_in, n_hid), bf16),
            pltpu.VMEM((n * cuts, n_hid, width), bf16),
            pltpu.VMEM((n_tok, n_hid), f32),
            pltpu.VMEM((n_tok, n_hid), f32),
            pltpu.VMEM((n_tok, n_hid), bf16),
            pltpu.VMEM((n * cuts, n_tok, width), bf16),
            pltpu.VMEM((nx * nb, n_tok, width), bf16),
            pltpu.VMEM((nx, nb, n_tok, width), bf16),
            pltpu.VMEM((nb, n_tok, width), f32),
            pltpu.VMEM((PIECES, 8, piece), f32),
            pltpu.VMEM((n_tp, PIECES, 8, piece), f32),
            dma((3 + cuts,)),
            dma((2, half, 2 + cuts)),
            dma((2, half, 2 + cuts)),
            dma((nx * nb, PIECES)),
            dma((nx * nb, PIECES)),
            dma((nx * nb, PIECES)),
            dma((nx, nb, PIECES)),
            dma((n_tp,)),
            dma((n_tp,)),
        ],
        compiler_params=pltpu.CompilerParams(
            collective_id=0, has_side_effects=True, vmem_limit_bytes=62 * 1024 * 1024
        ),
        name="ffn_ring",
    )(tokens, norm_gain[None, :], gate_weight, up_weight, down_weight, out_gain[None, :])


def line_order(k, nz):
    others = [s for s in range(nz) if s != k]
    return sorted(others, key=lambda s: (abs(s - k), abs(2 * s - nz + 1)))


def inward_order(k, nz):
    out = line_order(k, nz)
    if k in (0, nz - 1):
        out = out[1:] + out[:1]
    return out


def line_kernel(
    n, n_tp, tokens_hbm, norm_gain, gate_hbm, up_hbm, down_hbm, out_gain, out_hbm,
    result, tok, normed, gate, up, down, gate_acc, up_acc, hidden, parts, sib, near, far, own, squares, sq, sq_all,
    local_sem, y_send, y_recv, z_send, z_recv, tok_send, tok_recv,
    sib_send, sib_recv, near_send, near_recv, far_send, far_recv, sq_send, sq_recv, out_sem,
):
    nz = n // 2
    cuts = down.shape[0] // n
    nb = n * cuts // n_tp
    n_own, d_model = tok.shape
    rows_in, n_hid = gate.shape[1], gate.shape[2]
    width = down.shape[2]
    quarter = n_own // n_tp
    small = quarter // TOKEN_PIECES
    half_rows = n_own // PIECES
    fs, tp = lax.axis_index("fs"), lax.axis_index("tp")
    z, y = fs // 2, fs % 2
    x, core = tp // 2, tp % 2
    fs_y = z * 2 + 1 - y
    sibling, across = x * 2 + 1 - core, (1 - x) * 2 + core
    has_next = (z < nz - 1, z > 0)
    inner = (z > 0) & (z < nz - 1)
    outer = jnp.logical_not(inner)
    inward = jnp.where(z < nz // 2, 0, 1)

    barrier = pltpu.get_barrier_semaphore()
    pl.semaphore_signal(barrier, inc=1, device_id={"fs": fs_y}, device_id_type=MESH)
    for d in range(1, n_tp):
        pl.semaphore_signal(
            barrier, inc=1, device_id={"tp": (tp + d) % n_tp}, device_id_type=MESH
        )
    for way in (0, 1):

        @pl.when(has_next[way])
        def _():
            to = {"fs": fs + 2 - 4 * way}
            pl.semaphore_signal(barrier, inc=1, device_id=to, device_id_type=MESH)

    keep = pl.ds(pl.multiple_of(y * n_hid, n_hid), n_hid)
    give = pl.ds(pl.multiple_of((1 - y) * n_hid, n_hid), n_hid)
    loads = [
        pltpu.make_async_copy(tokens_hbm, tok, local_sem.at[0]),
        pltpu.make_async_copy(gate_hbm.at[:, keep], gate.at[fs], local_sem.at[1]),
        pltpu.make_async_copy(up_hbm.at[:, keep], up.at[fs], local_sem.at[2]),
    ]
    for j in range(cuts):
        cols = pl.ds(j * width, width)
        loads.append(
            pltpu.make_async_copy(
                down_hbm.at[keep, cols], down.at[fs * cuts + j], local_sem.at[3 + j]
            )
        )
    for load in loads:
        load.start()
    pl.semaphore_wait(barrier, n_tp + (z > 0).astype(jnp.int32) + (z < nz - 1).astype(jnp.int32))

    def shard(layer, other):
        return layer * 2 + (1 - y if other else y)

    def view(p, layer):
        if p < 4:
            return (gate, up)[p % 2].at[shard(layer, p // 2)]
        j = p - 4
        return down.at[layer * 2 * cuts + j]

    def z_copy(p, way, h, layer, src=None):
        dst = view(p, layer)
        return pltpu.make_async_remote_copy(
            src_ref=dst if src is None else src,
            dst_ref=dst,
            send_sem=z_send.at[way, h - 1, p],
            recv_sem=z_recv.at[way, h - 1, p],
            device_id={"fs": fs + 2 - 4 * way},
            device_id_type=MESH,
        )

    def send_own(p, where=None):
        src = (gate_hbm, up_hbm)[p].at[:, keep] if p < 2 else None
        for way in (0, 1):

            @pl.when(has_next[way] if where is None else has_next[way] & where(way))
            def _():
                z_copy(p, way, 1, z, src).start()

    order = [line_order(k, nz) for k in range(nz)]

    def pick(values):
        out = jnp.int32(values[0])
        for k in range(1, nz):
            out = jnp.where(z == k, values[k], out)
        return out

    sources = []
    for i in range(nz - 1):
        layer = pick([order[k][i] for k in range(nz)])
        way = pick([int(order[k][i] > k) for k in range(nz)])
        h = pick([abs(order[k][i] - k) for k in range(nz)])
        onward = pick([int(0 < k < nz - 1) for k in range(nz)]) == 1
        sources.append((layer, way, h, onward))

    def receive(i, p):
        layer, way, h, onward = sources[i]
        z_copy(p, way, h, layer).wait_recv()

        @pl.when(onward)
        def _():
            z_copy(p, way, h + 1, layer).start()

    def take(j):
        for i in range(nz - 1):
            if i != 1:
                receive(i, 4 + j)
        send_own(4 + j, lambda way: inward != way)

    def y_copy(p):
        if p < 2:
            src, dst = (gate_hbm, up_hbm)[p].at[:, give], (gate, up)[p]
            src, got = src, (gate, up)[p].at[fs_y]
            dst = (gate, up)[p].at[fs]
        elif p < 2 + cuts:
            j = p - 2
            src = down_hbm.at[give, pl.ds(j * width, width)]
            dst = down.at[fs * cuts + j]
        else:
            rows = token_rows(y, tp, p - 2 - cuts)
            src = dst = normed.at[:, rows]
        return pltpu.make_async_remote_copy(
            src_ref=src,
            dst_ref=dst,
            send_sem=y_send.at[p],
            recv_sem=y_recv.at[p],
            device_id={"fs": fs_y},
            device_id_type=MESH,
        )

    def token_rows(y_of, t, p):
        start = y_of * n_own + t * quarter + p * small
        return pl.ds(pl.multiple_of(start, small), small)

    def token_copy(kind, t, p, to):
        part = normed.at[:, token_rows(1 - y, t, p)]
        return pltpu.make_async_remote_copy(
            src_ref=part,
            dst_ref=part,
            send_sem=tok_send.at[kind, p],
            recv_sem=tok_recv.at[kind, p],
            device_id={"tp": to},
            device_id_type=MESH,
        )

    for p in (0, 1):
        send_own(p)
    for p in (0, 1):
        y_copy(p).start()

    loads[0].wait()
    tile = min(128, n_own)
    tiles = n_own // tile
    own_tiles = quarter // tile

    def normalize(i):
        rows = pl.ds(pl.multiple_of(i * tile, tile), tile)
        rows_to = pl.ds(pl.multiple_of(y * n_own + i * tile, tile), tile)
        v = tok[rows, :].astype(jnp.float32)
        r = lax.rsqrt(jnp.mean(v * v, axis=1, keepdims=True) + EPSILON)
        out = (v * r * norm_gain[...]).astype(jnp.bfloat16)
        for j in range(n):
            normed[j, rows_to, :] = out[:, j * rows_in:(j + 1) * rows_in]

    @pl.loop(0, own_tiles)
    def _(i):
        normalize(tp * own_tiles + i)

    for p in range(TOKEN_PIECES):
        y_copy(2 + cuts + p).start()
    for j in range(cuts):
        y_copy(2 + j).start()

    def accumulate(c, b, y_of, mode="mid"):
        weight, acc = (gate, up)[c], (gate_acc, up_acc)[c]
        step = min(COLUMN_TILE, n_hid)
        n_col = n_hid // step

        def part(half, i):
            rows = pl.ds(pl.multiple_of(half * n_own, n_own), n_own)
            cols = pl.ds(pl.multiple_of(i * step, step), step)
            v = jnp.dot(normed[b, rows, :], weight[b, :, cols], preferred_element_type=jnp.float32)
            if mode != "first":
                v = v + acc[rows, cols]
            if mode == "last":
                g = gate_acc[rows, cols]
                hidden[rows, cols] = (g * (1.0 / (1.0 + jnp.exp(-g))) * v).astype(jnp.bfloat16)
            else:
                acc[rows, cols] = v

        @pl.loop(0, n_col if y_of is not None else 2 * n_col)
        def _(i):
            part(*((y_of, i) if y_of is not None else (i // n_col, i % n_col)))

    def tokens_in(p):
        y_copy(2 + cuts + p).wait_recv()
        token_copy(0, tp, p, across).start()
        token_copy(1, tp, p, sibling).start()

    def tokens_on(p):
        token_copy(0, across, p, across).wait_recv()
        token_copy(2, across, p, sibling).start()

    @pl.loop(own_tiles, tiles // 2)
    def _(i):
        normalize((tp * own_tiles + i) % tiles)

    y_copy(0).wait_recv()
    send_own(2)

    @pl.loop(tiles // 2, tiles)
    def _(i):
        normalize((tp * own_tiles + i) % tiles)

    for load in loads[1:]:
        load.wait()
    y_copy(1).wait_recv()
    send_own(3)
    for p in (0, 1):
        receive(0, p)
    for c in (0, 1):
        accumulate(c, fs, y, "first")
    for p in range(TOKEN_PIECES // 2):
        tokens_in(p)
    for c in (0, 1):
        accumulate(c, fs_y, y)
    for p in (2, 3):
        receive(0, p)

    @pl.when(inner)
    def _():
        for i in range(1, nz - 2):
            for p in range(4):
                receive(i, p)

    for p in range(TOKEN_PIECES // 2, TOKEN_PIECES):
        tokens_in(p)
        tokens_on(p - TOKEN_PIECES // 2)
    for p in (0, 1):
        accumulate(p, shard(sources[0][0], 0), y)
    for j in range(cuts):
        y_copy(2 + j).wait_recv()
    for j in range(2 * cuts):
        send_own(4 + j, lambda way: outer)
    for j in range(2 * cuts):
        send_own(4 + j, lambda way: inner & (inward == way))
    for p in range(TOKEN_PIECES // 2, TOKEN_PIECES):
        tokens_on(p)
    for p in (0, 1):
        accumulate(p, shard(sources[0][0], 1), y)

    @pl.when(outer)
    def _():
        for i in range(1, nz - 2):
            for p in range(4):
                receive(i, p)

    for p in range(TOKEN_PIECES):
        token_copy(1, sibling, p, sibling).wait_recv()
        token_copy(2, across + 1 - 2 * core, p, sibling).wait_recv()

    last = nz - 2

    def receive_if(where, p):
        @pl.when(where)
        def _():
            receive(last, p)

    for p in range(3):
        receive_if(inner, p)

    for c in (0, 1):
        accumulate(c, fs, 1 - y, "first")
        accumulate(c, fs_y, 1 - y)
        for p in (0, 1):
            accumulate(c, shard(sources[0][0], p), 1 - y)
    receive_if(inner, 3)
    for i in range(1, nz - 2):
        for p in (0, 1):
            accumulate(p, shard(sources[i][0], 0), None)
    for i in range(1, nz - 2):
        for p in (0, 1):
            accumulate(p, shard(sources[i][0], 1), None)

    @pl.when(inner)
    def _():
        for j in range(2 * cuts):
            receive(1, 4 + j)

    receive_if(outer, 0)
    accumulate(0, shard(sources[last][0], 0), None)
    receive_if(outer, 1)
    accumulate(1, shard(sources[last][0], 0), None)
    receive_if(outer, 2)
    accumulate(0, shard(sources[last][0], 1), None)
    receive_if(outer, 3)

    accumulate(1, shard(sources[last][0], 1), None, "last")

    def owner(b):
        t = b // nb
        return t // 2, t % 2, b % nb

    def block_rows(q):
        return pl.ds(pl.multiple_of(q * n_own, n_own), n_own)

    def sib_copy(b, slot, q):
        return pltpu.make_async_remote_copy(
            src_ref=parts.at[b, block_rows(q)],
            dst_ref=sib.at[slot, block_rows(q)],
            send_sem=sib_send.at[slot, q],
            recv_sem=sib_recv.at[slot, q],
            device_id={"tp": sibling},
            device_id_type=MESH,
        )

    def part_rows(q, r):
        return pl.ds(pl.multiple_of(q * n_own + r * half_rows, half_rows), half_rows)

    def near_copy(b, q, r, slot, to):
        return pltpu.make_async_remote_copy(
            src_ref=parts.at[b, part_rows(q, r)],
            dst_ref=near.at[slot, part_rows(0, r)],
            send_sem=near_send.at[slot, r],
            recv_sem=near_recv.at[slot, r],
            device_id=to,
            device_id_type=MESH,
        )

    def far_copy(b, q, r, k, sent, to):
        return pltpu.make_async_remote_copy(
            src_ref=parts.at[b, part_rows(q, r)],
            dst_ref=far.at[k, part_rows(0, r)],
            send_sem=far_send.at[sent, r],
            recv_sem=far_recv.at[k, r],
            device_id=to,
            device_id_type=MESH,
        )

    to_y, to_x = {"fs": fs_y}, {"tp": across}

    def multiply(b):
        x_to, core_to, k = owner(b)

        @pl.loop(0, 2)
        def _(q):
            rows = block_rows(q)
            parts[b, rows, :] = jnp.dot(
                hidden[rows, :], down[b], preferred_element_type=jnp.float32
            ).astype(jnp.bfloat16)

            @pl.when(core_to != core)
            def _():
                sib_copy(b, x_to * nb + k, q).start()

    def fold(b, slot, q, r, extra=None):
        rows = part_rows(q, r)
        v = parts[b, rows, :].astype(jnp.float32) + sib[slot, rows, :].astype(jnp.float32)
        if extra is not None:
            v = v + near[extra, part_rows(0, r), :].astype(jnp.float32)
        parts[b, rows, :] = v.astype(jnp.bfloat16)

    def starts_on_y(x_to, core_to, k):
        same = x_to == z // (nz // 2)
        own_layer = x_to * 2 + core_to == z
        odd = (k + x_to + core_to) % 2 == 1
        return jnp.where(same, odd & (own_layer | (k != nb // 2)), odd | (k == nb - 1))

    def near_slot(y_first, x_to, k, q):
        return jnp.where(y_first, x_to, 2 + q) * nb + k

    def reduce(b):
        x_to, core_to, k = owner(b)
        y_first = starts_on_y(x_to, core_to, k)
        slot = x_to * nb + k

        @pl.when((core_to == core) & (y_first | (x_to != x)))
        def _():
            q = 1 - y
            to = {"fs": jnp.where(y_first, fs_y, fs), "tp": jnp.where(y_first, tp, across)}
            sib_copy(b, slot, q).wait_recv()
            for r in range(PIECES):
                fold(b, slot, q, r)
                near_copy(b, q, r, near_slot(y_first, x_to, k, q), to).start()

            @pl.when(jnp.logical_not(y_first))
            def _():
                sib_copy(b, slot, y).wait_recv()
                for r in range(PIECES):
                    fold(b, slot, y, r)
                    near_copy(b, y, r, near_slot(False, x_to, k, y), to_x).start()

    def pass_on(b):
        x_to, core_to, k = owner(b)
        y_first = starts_on_y(x_to, core_to, k)
        slot = x_to * nb + k

        @pl.when((core_to == core) & (y_first == (x_to != x)))
        def _():
            q = jnp.where(y_first, y, 1 - y)
            got = near_slot(y_first, x_to, k, q)
            to = {"fs": jnp.where(y_first, fs, fs_y), "tp": jnp.where(y_first, across, tp)}
            sib_copy(b, slot, q).wait_recv()
            for r in range(PIECES):
                near_copy(b, q, r, got, to_y).wait_recv()
                fold(b, slot, q, r, got)
                far_copy(b, q, r, k, slot, to).start()

    final_order = [[k] + inward_order(k, nz) for k in range(nz)]
    steps = []

    def run(b):
        m = len(steps)
        steps.append(b)
        multiply(b)
        if m >= 1:
            reduce(steps[m - 1])
        if m >= LAG:
            pass_on(steps[m - LAG])

    early = list(range(2 * cuts))

    def run_own(count):
        for j in early[:count]:
            run(z * 2 * cuts + j)
        del early[:count]

    def take_inner(j):
        if j < 2 * cuts:

            @pl.when(inner)
            def _():
                take(j)

    run_own(FIRST)
    take_inner(0)
    for j in range(2 * cuts):
        if j:
            take_inner(j + 1)
        for i in range(1, nz):
            layer = pick([final_order[k][i] for k in range(nz)])
            way = pick([int(final_order[k][i] > k) for k in range(nz)])
            h = pick([abs(final_order[k][i] - k) for k in range(nz)])

            @pl.when(outer)
            def _():
                z_copy(4 + j, way, h, layer).wait_recv()

            run(layer * 2 * cuts + j)
            if j == 0 and i == 1:
                take_inner(1)
            run_own(1)
    reduce(steps[-1])
    for b in steps[-LAG:]:
        pass_on(b)

    def piece_rows(q):
        return pl.ds(pl.multiple_of(q * half_rows, half_rows), half_rows)

    def out_copy(q):
        rows = piece_rows(q)
        return pltpu.make_async_copy(result.at[rows], out_hbm.at[rows], out_sem.at[q])

    for k in range(nb):
        slot = near_slot(starts_on_y(x, core, k), x, k, y)
        sib_copy(0, x * nb + k, y).wait_recv()
        for r in range(PIECES):
            near_copy(0, 0, r, slot, to_x).wait_recv()
        for r in range(PIECES):
            far_copy(0, 0, r, k, k, to_x).wait_recv()

        @pl.loop(0, n_own // tile)
        def _(i):
            rows = pl.ds(pl.multiple_of(i * tile, tile), tile)
            mine = pl.ds(pl.multiple_of(y * n_own + i * tile, tile), tile)
            v = parts[tp * nb + k, mine, :].astype(jnp.float32)
            v = v + sib[x * nb + k, mine, :].astype(jnp.float32)
            v = v + near[slot, rows, :].astype(jnp.float32)
            v = v + far[k, rows, :].astype(jnp.float32)
            own[k, rows, :] = v
            squares[rows, :] = v * v if k == 0 else squares[rows, :] + v * v

    for q in range(PIECES):
        total = jnp.sum(squares[piece_rows(q), :], axis=1, keepdims=True)
        sq[q] = jnp.transpose(jnp.broadcast_to(total, (half_rows, 128)))[0:8, :]

    def sq_copy(to, slot):
        return pltpu.make_async_remote_copy(
            src_ref=sq,
            dst_ref=sq_all.at[slot],
            send_sem=sq_send.at[to],
            recv_sem=sq_recv.at[slot],
            device_id={"tp": to},
            device_id_type=MESH,
        )

    others = [(tp + d) % n_tp for d in range(1, n_tp)]
    for t in others:
        sq_copy(t, tp).start()
    for p in range(2 + cuts + TOKEN_PIECES):
        y_copy(p).wait_send()
    for p in range(TOKEN_PIECES):
        token_copy(0, tp, p, across).wait_send()
        token_copy(1, tp, p, sibling).wait_send()
        token_copy(2, across, p, sibling).wait_send()
    for p in range(4 + 2 * cuts):
        for way in (0, 1):

            @pl.when(has_next[way])
            def _():
                z_copy(p, way, 1, z).wait_send()

        for layer, way, h, onward in sources:

            @pl.when(onward)
            def _():
                z_copy(p, way, h + 1, layer).wait_send()

    @pl.loop(0, 2)
    def _(q):
        for x_to in (0, 1):
            for k in range(nb):
                sib_copy(0, x_to * nb + k, q).wait_send()

    for x_to in (0, 1):
        for k in range(nb):
            y_first = starts_on_y(x_to, core, k)

            @pl.when(y_first)
            def _():
                for r in range(PIECES):
                    near_copy(0, 0, r, near_slot(True, x_to, k, 0), to_x).wait_send()

            @pl.when(jnp.logical_not(y_first) & (x_to != x))
            def _():
                for q in (0, 1):
                    for r in range(PIECES):
                        near_copy(0, 0, r, near_slot(False, x_to, k, q), to_x).wait_send()

            @pl.when(y_first == (x_to != x))
            def _():
                for r in range(PIECES):
                    far_copy(0, 0, r, k, x_to * nb + k, to_x).wait_send()

    for t in others:
        sq_copy(t, t).wait_recv()

    for q in range(PIECES):
        rows = piece_rows(q)
        total = sq[q]
        for t in others:
            total = total + sq_all[t, q]
        r = lax.rsqrt(total / d_model + EPSILON)
        r = jnp.transpose(jnp.broadcast_to(r[0:1, :], (128, half_rows)))
        for k in range(nb):
            cols = slice(k * width, (k + 1) * width)
            result[rows, cols] = (own[k, rows, :] * r * out_gain[:, cols]).astype(jnp.bfloat16)
        out_copy(q).start()
    for q in range(PIECES):
        out_copy(q).wait()

    for t in others:
        sq_copy(t, tp).wait_send()


def line_body(n, n_tp, tokens, norm_gain, gate_weight, up_weight, down_weight, out_gain):
    n_own, d_model = tokens.shape
    rows_in, n_hid = gate_weight.shape[0], gate_weight.shape[1] // 2
    cuts = max(down_weight.shape[1] // 128, 1)
    width = down_weight.shape[1] // cuts
    nz, nb = n // 2, n * cuts // n_tp
    n_tok = 2 * n_own
    bf16, f32 = jnp.bfloat16, jnp.float32
    dma = pltpu.SemaphoreType.DMA
    hbm = pl.BlockSpec(memory_space=pl.ANY)
    vmem = pl.BlockSpec(memory_space=pltpu.VMEM)
    return pl.pallas_call(
        functools.partial(line_kernel, n, n_tp),
        out_shape=jax.ShapeDtypeStruct((n_own, out_gain.shape[0]), bf16),
        in_specs=[hbm, vmem, hbm, hbm, hbm, vmem],
        out_specs=hbm,
        scratch_shapes=[
            pltpu.VMEM((n_own, out_gain.shape[0]), bf16),
            pltpu.VMEM((n_own, d_model), bf16),
            pltpu.VMEM((n, n_tok, rows_in), bf16),
            pltpu.VMEM((n, rows_in, n_hid), bf16),
            pltpu.VMEM((n, rows_in, n_hid), bf16),
            pltpu.VMEM((n * cuts, n_hid, width), bf16),
            pltpu.VMEM((n_tok, n_hid), f32),
            pltpu.VMEM((n_tok, n_hid), f32),
            pltpu.VMEM((n_tok, n_hid), bf16),
            pltpu.VMEM((n * cuts, n_tok, width), bf16),
            pltpu.VMEM((2 * nb, n_tok, width), bf16),
            pltpu.VMEM((4 * nb, n_own, width), bf16),
            pltpu.VMEM((nb, n_own, width), bf16),
            pltpu.VMEM((nb, n_own, width), f32),
            pltpu.VMEM((n_own, width), f32),
            pltpu.VMEM((PIECES, 8, n_own // PIECES), f32),
            pltpu.VMEM((n_tp, PIECES, 8, n_own // PIECES), f32),
            dma((3 + cuts,)),
            dma((2 + cuts + TOKEN_PIECES,)),
            dma((2 + cuts + TOKEN_PIECES,)),
            dma((2, nz - 1, 4 + 2 * cuts)),
            dma((2, nz - 1, 4 + 2 * cuts)),
            dma((3, TOKEN_PIECES)),
            dma((3, TOKEN_PIECES)),
            dma((2 * nb, 2)),
            dma((2 * nb, 2)),
            dma((4 * nb, PIECES)),
            dma((4 * nb, PIECES)),
            dma((2 * nb, PIECES)),
            dma((nb, PIECES)),
            dma((n_tp,)),
            dma((n_tp,)),
            dma((PIECES,)),
        ],
        compiler_params=pltpu.CompilerParams(
            collective_id=0, has_side_effects=True, vmem_limit_bytes=62 * 1024 * 1024
        ),
        name="ffn_line",
    )(tokens, norm_gain[None, :], gate_weight, up_weight, down_weight, out_gain[None, :])


def solution(mesh):
    n, n_tp = mesh.shape["fs"], mesh.shape["tp"]
    paired = n_tp == 4 and n % 2 == 0 and n // 2 > 2
    return jax.shard_map(
        functools.partial(line_body if paired else body, n, n_tp),
        mesh=mesh,
        in_specs=(P("fs", None), P(), P("fs", "tp"), P("fs", "tp"), P("tp", "fs"), P("tp")),
        out_specs=P("fs", "tp"),
        check_vma=False,
    )
```
